32 devices in a mesh: sp: 8 (over z, y), tp: 4 (over x, core).
Axes of the slice: x: 2, y: 2, z: 4, core: 2. Of those that a mesh axis runs over, the one named last changes fastest.
Arguments:
- head_queries: bfloat16 [2048, 2048], P('sp', 'tp'), may hold values from -6 to 6
- head_keys: bfloat16 [2048, 2048], P('sp', 'tp'), may hold values from -6 to 6
- head_values: bfloat16 [2048, 2048], P('sp', 'tp'), may hold values from -6 to 6
- decay_logits: bfloat16 [2048, 2048], P('sp', 'tp'), may hold values from -12 to 1
- learning_logits: bfloat16 [2048, 32], P('sp', 'tp'), may hold values from -9 to 2
- surge_decay: float32 [2048, 32], P('sp', 'tp'), may hold values from -0.7 to 0
- documents: int32 [2048], P('sp'), may hold values from 0 to 2, never falling along the last dimension, each value on 1 to 1536 neighbouring positions
- residual: bfloat16 [2048, 2048], P(('sp', 'tp')), may hold values from -6 to 6
- head_norm_scale: float32 [2048], P('tp'), may hold values from 0.1 to 1.9
- mixer_output_weight: bfloat16 [2048, 2048], P('tp'), may hold values from -0.125 to 0.125
- layer_norm_scale: float32 [2048], replicated, may hold values from 0.1 to 1.9
- routes: int32 [2048, 2], P('sp'), may hold values from 0 to 15, all different within a row; in each aligned block of 64 rows (0 to 63, 64 to 127, ...) at most 12 rows name the same one
- routing_weight: float32 [2048, 2], P(('sp', 'tp')), may hold values from 0.3 to 1.5
- routed_gate_weight: bfloat16 [16, 2048, 1024], P('sp', None, 'tp'), may hold values from -0.125 to 0.125
- routed_up_weight: bfloat16 [16, 2048, 1024], P('sp', None, 'tp'), may hold values from -0.125 to 0.125
- routed_down_weight: bfloat16 [16, 1024, 2048], P('sp', 'tp'), may hold values from -0.1875 to 0.1875
- common_gate_weight: bfloat16 [2048, 512], P(None, 'tp'), may hold values from -0.125 to 0.125
- common_up_weight: bfloat16 [2048, 512], P(None, 'tp'), may hold values from -0.125 to 0.125
- common_down_weight: bfloat16 [512, 2048], P('tp'), may hold values from -0.25 to 0.25
Outputs:
- layer_out: bfloat16 [2048, 2048], P(('sp', 'tp'))
The draws below stay inside these ranges and needn't reach their ends.
Inputs may be any that keep to these rules, and one draw needn't show every extreme that they name: `documents`: numbers never fall along the positions; each document holds 1 to 1536 positions and one holds exactly 1536. `routes`: each row names 2 different experts; in each aligned block of 64 rows no expert is named by more than 12 rows, a bound that some block reaches.
All inputs are finite; a program needn't handle non-finite values.
Results may differ from the reference program's by a relative error of at most 0.019.
Values may be sent and summed in bfloat16 or wider, within the bound.
A program may use at most 128 MiB of HBM per device.

```python
import math
import jax
import jax.numpy as jnp
import numpy as np
from jax import lax

D = 2048
HEAD_TOTAL = 32
HEAD = 64
FFE = 1024
SFF = 512
TOP = 2
TOK_DEV = 64
EXPERTS = 16
GROUP_TOK = 256
TOKEN_TOTAL = 2048
CAP = 12
DOCS = 3
DOC_MOST = 1536
SURGE_POSITIONS = 4
N_SP = 8
N_TP = 4


def slow_heads(key):
    slow_share = 0.5
    return jax.random.bernoulli(jax.random.fold_in(key, 11), slow_share, (HEAD_TOTAL,))


def draw_decay_logits(key, part):
    chosen = slow_heads(key)
    subkeys = jax.random.split(jax.random.fold_in(key, 21), 4)
    slow_level = math.log(0.3 / DOC_MOST) + 0.5
    head_level = jnp.where(chosen, slow_level, -2.95) + jax.random.uniform(subkeys[0], (HEAD_TOTAL,), jnp.float32, -0.3, 0.3)
    channel = jnp.repeat(head_level, HEAD) + jax.random.uniform(subkeys[1], (D,), jnp.float32, -0.3, 0.3)
    group_level = jnp.repeat(jax.random.uniform(subkeys[2], (TOKEN_TOTAL // GROUP_TOK,), jnp.float32, -0.4, 0.4), GROUP_TOK)
    data_part = 0.5 * jax.random.truncated_normal(subkeys[3], -4.0, 4.0, (TOKEN_TOTAL, D), jnp.float32)
    return (channel[None, :] + group_level[:, None] + data_part).astype(jnp.bfloat16)


def draw_learning_logits(key, part):
    chosen = slow_heads(key)
    subkeys = jax.random.split(jax.random.fold_in(key, 31), 3)
    slow_base = jax.random.uniform(subkeys[0], (HEAD_TOTAL,), jnp.float32, -7.0, -4.5)
    fast_base = jax.random.uniform(subkeys[1], (HEAD_TOTAL,), jnp.float32, -3.0, 0.0)
    base_level = jnp.where(chosen, slow_base, fast_base)
    data_part = 0.5 * jax.random.truncated_normal(subkeys[2], -4.0, 4.0, (TOKEN_TOTAL, HEAD_TOTAL), jnp.float32)
    return (base_level[None, :] + data_part).astype(jnp.bfloat16)


def draw_surge_decay(key, part):
    position_list = jax.random.permutation(jax.random.fold_in(key, 41), TOKEN_TOTAL)[:SURGE_POSITIONS].astype(jnp.int32)
    correction_scale = jax.random.uniform(jax.random.fold_in(key, 42), (SURGE_POSITIONS, HEAD_TOTAL), jnp.float32, 0.5, 0.8)
    hit_table = (jnp.arange(TOKEN_TOTAL, dtype=jnp.int32)[:, None] == position_list[None, :]).astype(jnp.float32)
    return jnp.dot(hit_table, jnp.log(correction_scale).astype(jnp.float32), precision=jax.lax.Precision.HIGHEST)


def level_of(key, dims, cuts, least, largest):
    factor_of, own = 1.0, jax.random.fold_in(key, 6)
    for axis_at, shards_of in cuts:
        steps = jnp.exp(jax.random.uniform(jax.random.fold_in(own, axis_at), (shards_of,), jnp.float32, least / len(cuts), largest / len(cuts)))
        factor_of = factor_of * jnp.repeat(steps, dims[axis_at] // shards_of).reshape([-1 if axis == axis_at else 1 for axis in range(len(dims))])
    return factor_of


def length_profile(count, total, bound, skew):
    weights = [(1 << 20) // math.isqrt(grade ** skew) + 1 for grade in range(2, count + 1)]
    spare, holding = total - bound - (count - 1), [1] * (count - 1)
    while spare > 0:
        free = [i for i in range(count - 1) if holding[i] < bound]
        whole, budget = sum([weights[i] for i in free]), spare
        for i in free:
            more = min(bound - holding[i], max(1, budget * weights[i] // whole), spare)
            holding[i] = holding[i] + more
            spare = spare - more
    return np.array([bound] + holding)


def ragged_sizes(key, amount, total, most, lean):
    if amount == 2:
        one = jax.random.randint(key, (), max(1, total - most), min(most, total - 1) + 1)
        return jnp.stack([one, total - one])
    lengths = jnp.asarray(length_profile(amount, total, most, lean), jnp.int32)
    pairs = (amount - 1) // 2
    donor, taker = lengths[1:1 + 2 * pairs:2], lengths[2:2 + 2 * pairs:2]
    room = jnp.minimum(donor - 1, most - taker)
    shifted = jax.random.randint(jax.random.fold_in(key, 1), (pairs,), 0, 1 << 20) % (room + 1)
    lengths = lengths.at[1:1 + 2 * pairs:2].set(donor - shifted).at[2:2 + 2 * pairs:2].set(taker + shifted)
    return lengths[jax.random.permutation(jax.random.fold_in(key, 2), amount)]


def assign_block(key, own, number, rows, number_of, top, reach, skew):
    order = jax.random.permutation(key, number_of)
    crowded, usual = shares(number_of, rows * top, reach, skew, True), shares(number_of, rows * top, reach, skew, False)
    places = jnp.arange(number_of)

    def named(lengths, turn):
        used = int((lengths > 0).sum())
        fixed = max(1, used // 4)
        moved = fixed + (places - fixed + turn * (used - fixed)) % max(1, number_of - fixed)
        return jnp.zeros((number_of,), jnp.int32).at[order[jnp.where(places < fixed, places, moved)]].set(jnp.asarray(lengths, jnp.int32))

    lengths = jnp.where(number % 4 == 0, named(crowded, number // 4), named(usual, number - number // 4 - 1))
    mixed = jax.random.permutation(jax.random.fold_in(own, 3), number_of)
    giver, receiver = mixed[0:number_of // 2 * 2:2], mixed[1:number_of // 2 * 2:2]
    room = jnp.minimum(lengths[giver] - 1, reach - lengths[receiver]) // 2
    room = jnp.where((giver == order[0]) | (receiver == order[0]) | (lengths[receiver] == 0), 0, jnp.maximum(room, 0))
    moved = jax.random.randint(jax.random.fold_in(own, 4), (number_of // 2,), 0, 1 << 20) % (room + 1)
    lengths = lengths.at[giver].add(-moved).at[receiver].add(moved)
    members = jnp.searchsorted(jnp.cumsum(lengths), jnp.arange(rows * top), side="right").astype(jnp.int32)
    grid = members.reshape(top, rows).T
    grid = grid[jax.random.permutation(jax.random.fold_in(own, 1), rows)]
    turn = jax.random.randint(jax.random.fold_in(own, 2), (rows, 1), 0, top)
    return jnp.take_along_axis(grid, (jnp.arange(top)[None, :] + turn) % top, axis=1)


def shares(number_of, total, reach, slope, full):
    loads = [(1 << 20) // math.isqrt(rank ** slope) + 1 for rank in range(1, number_of + 1)]
    largest = reach if full else min(reach, max(-(-total // number_of), total * loads[0] // sum(loads)))
    least = 1 if total - largest >= number_of - 1 else 0
    given, rest = [largest] + [least] * (number_of - 1), total - largest - least * (number_of - 1)
    while rest > 0:
        movable = [i for i in range(1, number_of) if given[i] < largest] or [i for i in range(1, number_of) if given[i] < reach]
        whole, budget = sum([loads[i] for i in movable]), rest
        for i in movable:
            addition = min(reach - given[i], max(1, budget * loads[i] // whole), rest)
            given[i] = given[i] + addition
            rest = rest - addition
    return np.array(given)


def normal_values(rng, dims, deviation, reach, cuts=(), held_as=jnp.bfloat16):
    level = level_of(rng, dims, cuts, -0.22, 0.18) if cuts else 1.0
    drawn = jax.random.normal(rng, dims, jnp.float32) * deviation * level
    return jnp.minimum(jnp.maximum(drawn, -reach), reach).astype(held_as)


def setup_inputs(seed: int = 0) -> dict:
    keys = jax.random.split(jax.random.key(seed), 20)
    head_queries = normal_values(keys[0], (TOKEN_TOTAL, D), 1.0, 6.0, ((0, 8), (1, 4)))
    head_keys = normal_values(keys[1], (TOKEN_TOTAL, D), 1.0, 6.0, ((0, 8), (1, 4)))
    head_values = normal_values(keys[2], (TOKEN_TOTAL, D), 1.0, 6.0, ((0, 8), (1, 4)))
    decay_logits = draw_decay_logits(jax.random.fold_in(keys[19], 71), 0)
    learning_logits = draw_learning_logits(jax.random.fold_in(keys[19], 71), 0)
    surge_decay = draw_surge_decay(jax.random.fold_in(keys[19], 71), 0)
    documents = jnp.searchsorted(jnp.cumsum(ragged_sizes(keys[6], DOCS, TOKEN_TOTAL, DOC_MOST, 1)), jnp.arange(TOKEN_TOTAL), side="right").astype(jnp.int32)
    residual = normal_values(keys[7], (TOKEN_TOTAL, D), 1.0, 6.0, ((0, 32),))
    head_norm_scale = jnp.clip(1.0 + 0.18 * jax.random.normal(keys[8], (D,), jnp.float32), 0.1, 1.9)
    mixer_output_weight = normal_values(keys[9], (D, D), D ** -0.5, 0.125, ((0, 4),))
    layer_norm_scale = jnp.clip(1.0 + 0.18 * jax.random.normal(keys[10], (D,), jnp.float32), 0.1, 1.9)
    routes_keys = jax.random.split(jax.random.fold_in(keys[11], 1), TOKEN_TOTAL // TOK_DEV)
    routes_turns = jax.random.permutation(jax.random.fold_in(keys[11], 3), TOKEN_TOTAL // TOK_DEV)
    routes = jax.vmap(lambda own, number: assign_block(jax.random.fold_in(keys[11], 2), own, number, TOK_DEV, EXPERTS, TOP, CAP, 2))(routes_keys, routes_turns).reshape((TOKEN_TOTAL, TOP))
    routing_weight = jnp.clip(jnp.exp(math.log(1.5) - 1.60943787 * jax.random.uniform(keys[12], (TOKEN_TOTAL, TOP), jnp.float32) ** level_of(keys[12], (TOKEN_TOTAL, TOP), ((0, 32),), -0.2, 0.2)), 0.3, 1.5)
    routed_gate_weight = normal_values(keys[13], (EXPERTS, D, FFE), D ** -0.5, 0.125, ((0, 8), (2, 4)))
    routed_up_weight = normal_values(keys[14], (EXPERTS, D, FFE), D ** -0.5, 0.125, ((0, 8), (2, 4)))
    routed_down_weight = normal_values(keys[15], (EXPERTS, FFE, D), FFE ** -0.5, 0.1875, ((0, 8), (1, 4)))
    common_gate_weight = normal_values(keys[16], (D, SFF), D ** -0.5, 0.125, ((1, 4),))
    common_up_weight = normal_values(keys[17], (D, SFF), D ** -0.5, 0.125, ((1, 4),))
    common_down_weight = normal_values(keys[18], (SFF, D), SFF ** -0.5, 0.25, ((0, 4),))
    return dict(head_queries=head_queries, head_keys=head_keys, head_values=head_values, decay_logits=decay_logits, learning_logits=learning_logits, surge_decay=surge_decay, documents=documents, residual=residual, head_norm_scale=head_norm_scale, mixer_output_weight=mixer_output_weight, layer_norm_scale=layer_norm_scale, routes=routes, routing_weight=routing_weight, routed_gate_weight=routed_gate_weight, routed_up_weight=routed_up_weight, routed_down_weight=routed_down_weight, common_gate_weight=common_gate_weight, common_up_weight=common_up_weight, common_down_weight=common_down_weight)


residual_scale = 2.0 ** 0.5
group_eps = 0.00064
norm_eps = 1e-05
unit_eps = 1e-06
highest = lax.Precision.HIGHEST

def linear_recurrence_mixer(head_queries, head_keys, head_values, decay_logits, learning_logits, surge_decay, documents, head_norm_scale):
    shape_three = (TOKEN_TOTAL, HEAD_TOTAL, HEAD)
    read_heads = head_queries.astype(jnp.float32).reshape(shape_three)
    key_heads = head_keys.astype(jnp.float32).reshape(shape_three)
    value_heads = head_values.astype(jnp.float32).reshape(shape_three)
    unit_keys = key_heads * lax.rsqrt(lax.optimization_barrier(jnp.sum(key_heads * key_heads, -1, keepdims=True)) + unit_eps)
    learn_rate = jax.nn.sigmoid(learning_logits.astype(jnp.float32))
    decay_logarithm = (-jnp.exp(-jax.nn.softplus(-decay_logits.astype(jnp.float32)) - 0.5)).reshape(shape_three)
    decay_logarithm = decay_logarithm + surge_decay[:, :, None]
    keeping = jnp.concatenate([jnp.zeros((1,), jnp.float32), (documents[1:] == documents[:-1]).astype(jnp.float32)])

    def advance(carried, inputs):
        read_now, key_now, value_now, unit_now, rate_now, decay_now, keep_now = inputs
        pulled = jnp.einsum('hvk,hk->hv', carried, unit_now, precision=highest)
        carried = keep_now * (carried * jnp.exp(decay_now)[:, None, :] - (rate_now[:, None] * pulled)[:, :, None] * unit_now[:, None, :])
        carried = carried + value_now[:, :, None] * key_now[:, None, :]
        return (carried, jnp.einsum('hvk,hk->hv', carried, read_now, precision=highest))
    initial = jnp.zeros((HEAD_TOTAL, HEAD, HEAD), jnp.float32)
    _, head_read = lax.scan(advance, initial, (read_heads, key_heads, value_heads, unit_keys, learn_rate, decay_logarithm, keeping))
    centre = lax.optimization_barrier(jnp.mean(head_read, -1, keepdims=True))
    spread = lax.optimization_barrier(jnp.mean(jnp.square(head_read - centre), -1, keepdims=True))
    normed = ((head_read - centre) * lax.rsqrt(spread + group_eps)).reshape(TOKEN_TOTAL, D) * head_norm_scale
    return normed.astype(jnp.bfloat16)

def rounded(values):
    return lax.optimization_barrier(values.astype(jnp.bfloat16)).astype(jnp.float32)

def split_down(hidden, down):
    block_width = hidden.shape[1] // N_TP
    pieces = jnp.einsum('rjf,jfd->jrd', hidden.reshape(hidden.shape[0], N_TP, block_width).astype(jnp.float32), down.reshape(N_TP, block_width, D).astype(jnp.float32))
    return lax.optimization_barrier(jnp.sum(rounded(pieces), 0))

def swiglu_hidden(rows_in, gate, upward):
    gated = jnp.dot(rows_in, gate, preferred_element_type=jnp.float32)
    lifted = jnp.dot(rows_in, upward, preferred_element_type=jnp.float32)
    return (jax.nn.silu(gated) * lifted).astype(jnp.bfloat16)

def reference(head_queries, head_keys, head_values, decay_logits, learning_logits, surge_decay, documents, residual, head_norm_scale, mixer_output_weight, layer_norm_scale, routes, routing_weight, routed_gate_weight, routed_up_weight, routed_down_weight, common_gate_weight, common_up_weight, common_down_weight):
    head_outputs = linear_recurrence_mixer(head_queries, head_keys, head_values, decay_logits, learning_logits, surge_decay, documents, head_norm_scale)
    block_width = D // N_TP
    mixed_rows = jnp.zeros((TOKEN_TOTAL, D), jnp.float32)
    for block_index in range(N_TP):
        lower = block_index * block_width
        mixed_rows = mixed_rows + rounded(jnp.dot(head_outputs[:, lower:lower + block_width], mixer_output_weight[lower:lower + block_width], preferred_element_type=jnp.float32))
    summed = residual_scale * residual.astype(jnp.float32) + mixed_rows
    centre = lax.optimization_barrier(jnp.mean(summed, -1, keepdims=True))
    spread = lax.optimization_barrier(jnp.mean(jnp.square(summed - centre), -1, keepdims=True))
    stream = ((summed - centre) * lax.rsqrt(spread + norm_eps) * layer_norm_scale).astype(jnp.bfloat16)
    devices = N_SP * N_TP
    chosen = routes.reshape(devices, TOK_DEV * TOP)
    onehot = (chosen[..., None] == jnp.arange(EXPERTS, dtype=jnp.int32)).astype(jnp.int32)
    ranking = (lax.optimization_barrier(jnp.sum(jnp.cumsum(onehot, 1) * onehot, -1)) - 1).astype(jnp.int32)
    device_ids = jnp.arange(devices, dtype=jnp.int32)[:, None]
    slot_index = (chosen * (devices * CAP) + device_ids * CAP + ranking).reshape(-1).astype(jnp.int32)
    buffer = jnp.zeros((EXPERTS * devices * CAP, D), jnp.bfloat16).at[slot_index].set(jnp.repeat(stream, TOP, axis=0))

    def one_expert(operands):
        rows_in, gate, upward, down = operands
        return split_down(swiglu_hidden(rows_in, gate, upward), down).astype(jnp.bfloat16)
    results = lax.map(one_expert, (buffer.reshape(EXPERTS, devices * CAP, D), routed_gate_weight, routed_up_weight, routed_down_weight))
    picked = results.reshape(EXPERTS * devices * CAP, D)[slot_index].astype(jnp.float32).reshape(TOKEN_TOTAL, TOP, D)
    routed = lax.optimization_barrier(jnp.sum(picked * routing_weight[:, :, None], 1))

    def shared_block(rows_in):
        return split_down(swiglu_hidden(rows_in, common_gate_weight, common_up_weight), common_down_weight)
    shared_rows = lax.map(shared_block, stream.reshape(N_SP, TOKEN_TOTAL // N_SP, D)).reshape(TOKEN_TOTAL, D)
    return (residual_scale * stream.astype(jnp.float32) + routed + shared_rows).astype(jnp.bfloat16)
```

```python
import jax
import jax.numpy as jnp
from jax import lax
from jax.experimental import pallas as pl
from jax.experimental.pallas import tpu as pltpu
from jax.sharding import PartitionSpec as P

HEAD = 64
EXP_DEV = 2
TOP = 2
BLOCK_SPAN = 64
TOK_DEV = 64


residual_scale = 2.0**0.5
group_eps = 0.00064
norm_eps = 1e-05
unit_eps = 1e-06
SCORE_PRECISION = lax.Precision.HIGH


MESH = pl.DeviceIdType.MESH
VMEM = pl.BlockSpec(memory_space=pltpu.VMEM)


def remote(src, dst, send_sem, recv_sem, axis, index):
    return pltpu.make_async_remote_copy(
        src_ref=src,
        dst_ref=dst,
        send_sem=send_sem,
        recv_sem=recv_sem,
        device_id={axis: index},
        device_id_type=MESH,
    )


def greet(groups):
    barrier = pltpu.get_barrier_semaphore()
    count = 0
    for axis, size in groups:
        me = lax.axis_index(axis)
        for step in range(1, size):
            pl.semaphore_signal(
                barrier,
                inc=1,
                device_id={axis: lax.rem(me + step, size)},
                device_id_type=MESH,
            )
            count += 1
    pl.semaphore_wait(barrier, count)


def chunk_iota(rows, cols, dim):
    return lax.broadcasted_iota(jnp.int32, (rows, cols), dim)


def mm(left, right, precision=None):
    return jnp.dot(left, right, preferred_element_type=jnp.float32, precision=precision)


def mm_nt(left, right, precision=None):
    return lax.dot_general(
        left,
        right,
        (((1,), (1,)), ((), ())),
        preferred_element_type=jnp.float32,
        precision=precision,
    )


def mm_tn(left, right, precision=None):
    return lax.dot_general(
        left,
        right,
        (((0,), (0,)), ((), ())),
        preferred_element_type=jnp.float32,
        precision=precision,
    )


def narrow(values):
    return values.astype(jnp.bfloat16)


def split(values):
    top = narrow(values)
    return top, narrow(values - top.astype(jnp.float32))


def mixer_kernel(
    size,
    queries,
    keys,
    values,
    decays,
    rates,
    surges,
    docs,
    scale,
    out,
    unit_s,
    ahead_s,
    fwd_s,
    reads_s,
    solved_s,
    map_s,
    add_s,
    local_s,
    starts_s,
    comp_s,
    far_s,
    join_s,
    doc_out,
    doc_in,
    padd_out,
    padd_in,
    pmap_out,
    pmap_in,
    s_out,
    s_in,
    doc_sem,
    padd_sem,
    pmap_sem,
    near_sem,
    next_sem,
    s_recv,
):
    me = lax.axis_index("sp")
    span = BLOCK_SPAN
    rows, width = queries.shape
    chunks = rows // span
    lanes = 2 * HEAD
    pairs = width // lanes
    heads = rates.shape[1]
    high = lax.Precision.HIGH
    barrier = pltpu.get_barrier_semaphore()
    for step in (1, 2, size - 1, size - 2):
        pl.semaphore_signal(
            barrier, inc=1, device_id={"sp": lax.rem(me + step, size)}, device_id_type=MESH
        )

    same_half = (chunk_iota(lanes, lanes, 0) // HEAD) == (chunk_iota(lanes, lanes, 1) // HEAD)
    ones_half = same_half.astype(jnp.float32)
    earlier = lax.rem(chunk_iota(span, lanes, 1), HEAD)
    later = chunk_iota(span, lanes, 0)
    unit_pair = (earlier == later).astype(jnp.float32)
    unit_full = (chunk_iota(lanes, lanes, 0) == chunk_iota(lanes, lanes, 1)).astype(jnp.float32)

    def wide(block):
        return jnp.where(same_half, jnp.concatenate([block, block], 0), 0.0)

    row_docs = docs[...].astype(jnp.float32)
    row_square = jnp.broadcast_to(row_docs, (rows, rows))
    diag = chunk_iota(rows, rows, 0) == chunk_iota(rows, rows, 1)
    doc_col = mm(
        narrow(jnp.where(diag, row_square, 0.0)), jnp.ones((rows, lanes), jnp.bfloat16)
    )
    pick = (
        lax.rem(chunk_iota(rows, lanes, 0), span) == lax.rem(chunk_iota(rows, lanes, 1), HEAD)
    ).astype(jnp.bfloat16)
    wide_rows = 8 * ((chunks + 7) // 8)
    in_chunk = (chunk_iota(wide_rows, rows, 1) // span) == chunk_iota(wide_rows, rows, 0)
    doc_row = mm(
        narrow(jnp.where(in_chunk, jnp.broadcast_to(row_docs, (wide_rows, rows)), 0.0)), pick
    )
    same_chunk = (chunk_iota(rows, rows, 0) // span) == (chunk_iota(rows, rows, 1) // span)
    tri = (
        (chunk_iota(rows, rows, 0) >= chunk_iota(rows, rows, 1)) & same_chunk
    ).astype(jnp.bfloat16)

    strict, causal, joined, tail = [], [], [], []
    for c in range(chunks):
        col = doc_col[c * span : (c + 1) * span]
        same_doc = col == doc_row[c : c + 1]
        strict.append(same_doc & (later > earlier))
        causal.append(same_doc & (later >= earlier))
        before_row = doc_col[max(c * span - 1, 0) : max(c * span - 1, 0) + 1]
        joined.append((col == before_row).astype(jnp.float32))
        tail.append((col == doc_col[(c + 1) * span - 1 : (c + 1) * span]).astype(jnp.float32))

    doc_out[...] = jnp.broadcast_to(doc_col[rows - 1 : rows], doc_out.shape)
    pl.semaphore_wait(barrier, 4)
    following = lax.rem(me + 1, size)
    doc_hop = remote(doc_out, doc_in, doc_sem.at[0], doc_sem.at[1], "sp", following)

    @pl.when(me < size - 1)
    def _():
        doc_hop.start()

    rate_all = jax.nn.sigmoid(rates[...].astype(jnp.float32))
    surge_all = surges[...]

    def local_pairs(turn, carry):
        streams = []
        for half in range(2):
            p = turn * 2 + half
            cols = pl.ds(pl.multiple_of(p * lanes, lanes), lanes)
            spread_heads = (
                chunk_iota(heads, lanes, 0) == 2 * p + chunk_iota(heads, lanes, 1) // HEAD
            ).astype(jnp.float32)
            key = keys[:, cols].astype(jnp.float32)
            norm = mm(key * key, ones_half, high)
            unit = key * lax.rsqrt(norm + unit_eps)
            rate = mm(rate_all, spread_heads, high)
            surge = mm(surge_all, spread_heads, high)
            logit = decays[:, cols].astype(jnp.float32)
            decay = surge - jnp.exp(-0.5) / (1.0 + jnp.exp(-logit))
            top, rest = split(decay)
            cumulative = mm(tri, top) + mm(tri, rest)
            grown = jnp.exp(cumulative)
            shrunk = jnp.exp(-cumulative)
            ahead = unit * jnp.exp(cumulative - decay)
            unit_rate = unit * rate
            back_unit = unit_rate * shrunk
            back_key = key * shrunk
            forward = queries[:, cols].astype(jnp.float32) * grown
            ahead_s[:, cols] = ahead
            fwd_s[:, cols] = forward
            for c in range(chunks):
                part = slice(c * span, (c + 1) * span)
                total = cumulative[(c + 1) * span - 1 : (c + 1) * span]
                ending = jnp.exp(total - cumulative[part]) * tail[c]
                streams.append(
                    dict(
                        c=c,
                        p=p,
                        cols=cols,
                        ahead=ahead[part],
                        fwd=forward[part],
                        bu=back_unit[part],
                        bk=back_key[part],
                        eu=-unit_rate[part] * ending,
                        ek=key[part] * ending,
                        val=values[part, cols].astype(jnp.float32),
                        keep=jnp.exp(total) * joined[c][span - 1 : span],
                    )
                )
        for s in streams:
            c = s["c"]
            scores = mm_nt(
                jnp.concatenate([s["ahead"], s["fwd"]], 0),
                jnp.concatenate([wide(s["bu"]), wide(s["bk"])], 0),
                SCORE_PRECISION,
            )
            s["low"] = jnp.where(strict[c], scores[:span, :lanes], 0.0)
            s["mixk"] = jnp.where(strict[c], scores[:span, lanes:], 0.0)
            reads_s[c, s["p"], :, :lanes] = narrow(
                jnp.where(causal[c], -scores[span:, :lanes], 0.0)
            )
            reads_s[c, s["p"], :, lanes:] = narrow(jnp.where(causal[c], scores[span:, lanes:], 0.0))
        base = 16
        near_block = (earlier // base) == (later // base)
        for s in streams:
            s["low_near"] = jnp.where(near_block, s["low"], 0.0)
            s["inv"] = unit_pair - s["low_near"]
        for s in streams:
            s["power"] = mm(s["low_near"], wide(s["low_near"]), high)
            s["mv"] = mm(s["mixk"], wide(s["val"]))
        reach = 2
        while reach < base:
            last = reach * 2 >= base
            for s in streams:
                right = wide(s["power"])
                if last:
                    s["inv"] = s["inv"] + mm(s["inv"], right, high)
                else:
                    both = mm(jnp.concatenate([s["power"], s["inv"]], 0), right, high)
                    s["power"] = both[:span]
                    s["inv"] = s["inv"] + both[span:]
            reach = reach * 2
        while base < span:
            off = ((earlier // base) != (later // base)) & (
                (earlier // (2 * base)) == (later // (2 * base))
            )
            for s in streams:
                s["mid"] = mm(s["inv"], wide(jnp.where(off, s["low"], 0.0)), high)
            for s in streams:
                s["inv"] = s["inv"] - mm(s["mid"], wide(s["inv"]), high)
            base = base * 2
        for s in streams:
            c = s["c"]
            s["solved"] = mm(
                s["inv"],
                jnp.concatenate([wide(s["ahead"] * joined[c]), wide(s["mv"])], 1),
                high,
            )
            solved_s[c, s["p"]] = narrow(s["solved"])
        for s in streams:
            c, p = s["c"], s["p"]
            pull = mm_tn(s["solved"][:, :lanes], s["eu"], high)
            map_s[c, p] = jnp.where(same_half, pull, 0.0) + unit_full * s["keep"]
            grown = mm_tn(
                jnp.concatenate([s["solved"][:, lanes:], s["val"]], 0),
                jnp.concatenate([s["eu"], s["ek"]], 0),
                high,
            )
            grown = jnp.where(same_half, grown, 0.0)
            add_s[c, p] = grown[:HEAD] + grown[HEAD:]
        return carry

    lax.fori_loop(0, pairs // 2, local_pairs, 0)

    state = [None] * pairs
    for p in range(pairs):
        state[p] = jnp.concatenate([add_s[0, p], map_s[0, p][:HEAD] + map_s[0, p][HEAD:]], 0)
    kept = [state]
    for c in range(1, chunks):
        state = [
            mm(kept[-1][p], map_s[c, p], high)
            + jnp.concatenate([add_s[c, p], jnp.zeros((HEAD, lanes), jnp.float32)], 0)
            for p in range(pairs)
        ]
        kept.append(state)
    finals = kept[-1]

    @pl.when(me == 0)
    def _():
        join_s[...] = jnp.zeros_like(join_s)
        s_in[...] = jnp.zeros_like(s_in)

    @pl.when(me > 0)
    def _():
        doc_hop.wait_recv()
        join_s[...] = (doc_in[...] == doc_col[0:1]).astype(jnp.float32)

    join = join_s[0:1]
    for p in range(pairs):
        comp_s[p] = jnp.concatenate([finals[p][:HEAD], finals[p][HEAD:] * join], 0)
    even = lax.rem(me, 2) == 0

    def pair_hop(p):
        return (
            remote(padd_out.at[p], padd_in.at[p], padd_sem.at[0, p], padd_sem.at[1, p], "sp", following),
            remote(pmap_out.at[p], pmap_in.at[p], pmap_sem.at[0, p], pmap_sem.at[1, p], "sp", following),
        )

    def state_hop(p, near):
        sem = near_sem if near else next_sem
        return remote(
            s_out.at[p],
            s_in.at[p],
            sem.at[p],
            s_recv.at[p],
            "sp",
            lax.rem(me + (2 if near else 1), size),
        )

    @pl.when(even)
    def _():
        for p in range(pairs):
            padd_out[p] = narrow(comp_s[p, :HEAD])
            pmap_out[p] = comp_s[p, HEAD:]
        for p in range(pairs):
            pair_hop(p)[0].start()
        for p in range(pairs):
            pair_hop(p)[1].start()

    def finish_local():
        for p in range(pairs):
            cols = slice(p * lanes, (p + 1) * lanes)
            for c in range(chunks):
                part = slice(c * span, (c + 1) * span)
                read_unit = reads_s[c, p, :, :lanes]
                solved = solved_s[c, p].astype(jnp.float32)
                local = mm(
                    reads_s[c, p],
                    jnp.concatenate(
                        [
                            narrow(wide(solved[:, lanes:])),
                            narrow(wide(values[part, cols].astype(jnp.float32))),
                        ],
                        0,
                    ),
                )
                start = fwd_s[part, cols] * joined[c] + mm(
                    read_unit, narrow(wide(solved[:, :lanes]))
                )
                if c > 0:
                    seen = mm_nt(
                        narrow(start),
                        jnp.concatenate(
                            [
                                narrow(wide(kept[c - 1][p][:HEAD])),
                                narrow(wide(kept[c - 1][p][HEAD:])),
                            ],
                            0,
                        ),
                    )
                    local = local + seen[:, :lanes]
                    start = seen[:, lanes:]
                local_s[part, cols] = local
                starts_s[part, cols] = narrow(start)

    finish_local()

    @pl.when(jnp.logical_not(even))
    def _():
        for p in range(pairs):
            pair_hop(p)[0].wait_recv()
            first = padd_in[p]
            top, rest = split(wide(comp_s[p, HEAD:]))
            far_s[p, :HEAD] = (
                mm(jnp.concatenate([first, first], 1), jnp.concatenate([top, rest], 0))
                + comp_s[p, :HEAD]
            )

        @pl.when(me == 1)
        def _():
            s_in[...] = jnp.zeros_like(s_in)
            for p in range(pairs):
                s_out[p] = narrow(far_s[p, :HEAD])
                state_hop(p, True).start()

        for p in range(pairs):
            pair_hop(p)[1].wait_recv()

        @pl.when(me > 1)
        def _():
            for p in range(pairs):
                both = mm(pmap_in[p], wide(comp_s[p, HEAD:]), high)
                far_s[p, HEAD:] = both
            weights = []
            for p in range(pairs):
                top, rest = split(wide(far_s[p, HEAD:]))
                weights.append(jnp.concatenate([top, rest], 0))
            for p in range(pairs):
                state_hop(p, True).wait_recv()

                @pl.when(me < size - 1)
                def _():
                    arrived = s_in[p]
                    s_out[p] = narrow(
                        mm(jnp.concatenate([arrived, arrived], 1), weights[p]) + far_s[p, :HEAD]
                    )
                    state_hop(p, True).start()

        @pl.when(me < size - 1)
        def _():
            for p in range(pairs):
                state_hop(p, False).start()

        for p in range(pairs):
            top, rest = split(wide(pmap_in[p]))
            arrived = s_in[p]
            comp_s[p, :HEAD] = (
                mm(jnp.concatenate([arrived, arrived], 1), jnp.concatenate([top, rest], 0))
                + padd_in[p].astype(jnp.float32)
            )

    @pl.when(even)
    def _():
        @pl.when(me > 0)
        def _():
            for p in range(pairs):
                state_hop(p, False).wait_recv()

        for p in range(pairs):
            comp_s[p, :HEAD] = s_in[p].astype(jnp.float32)

    for p in range(pairs):
        cols = slice(p * lanes, (p + 1) * lanes)
        incoming = narrow(wide(comp_s[p, :HEAD] * join))
        read = local_s[:, cols] + mm_nt(starts_s[:, cols], incoming)
        centred = read - mm(read, ones_half, high) * (1.0 / HEAD)
        spread = mm(centred * centred, ones_half, high) * (1.0 / HEAD)
        out[:, cols] = narrow(centred * lax.rsqrt(spread + group_eps) * scale[:, cols])

    @pl.when(me < size - 1)
    def _():
        doc_hop.wait_send()

    @pl.when(even)
    def _():
        for p in range(pairs):
            for hop in pair_hop(p):
                hop.wait_send()

    @pl.when(jnp.logical_not(even) & (me < size - 1))
    def _():
        for p in range(pairs):
            state_hop(p, True).wait_send()
            state_hop(p, False).wait_send()


def mixer(queries, keys, values, decays, rates, surges, documents, scale):
    size = lax.axis_size("sp")
    rows, width = queries.shape
    lanes = 2 * HEAD
    pairs = width // lanes
    chunks = rows // BLOCK_SPAN
    f32, b16 = jnp.float32, jnp.bfloat16
    dma = pltpu.SemaphoreType.DMA
    return pl.pallas_call(
        lambda *refs: mixer_kernel(size, *refs),
        out_shape=jax.ShapeDtypeStruct((rows, width), b16),
        in_specs=[VMEM] * 8,
        out_specs=VMEM,
        scratch_shapes=[
            pltpu.VMEM((8, lanes), f32),
            pltpu.VMEM((rows, width), f32),
            pltpu.VMEM((rows, width), f32),
            pltpu.VMEM((chunks, pairs, BLOCK_SPAN, 2 * lanes), b16),
            pltpu.VMEM((chunks, pairs, BLOCK_SPAN, 2 * lanes), b16),
            pltpu.VMEM((chunks, pairs, lanes, lanes), f32),
            pltpu.VMEM((chunks, pairs, HEAD, lanes), f32),
            pltpu.VMEM((rows, width), f32),
            pltpu.VMEM((rows, width), b16),
            pltpu.VMEM((pairs, lanes, lanes), f32),
            pltpu.VMEM((pairs, lanes, lanes), f32),
            pltpu.VMEM((8, lanes), f32),
            pltpu.VMEM((8, lanes), f32),
            pltpu.VMEM((8, lanes), f32),
            pltpu.VMEM((pairs, HEAD, lanes), b16),
            pltpu.VMEM((pairs, HEAD, lanes), b16),
            pltpu.VMEM((pairs, HEAD, lanes), f32),
            pltpu.VMEM((pairs, HEAD, lanes), f32),
            pltpu.VMEM((pairs, HEAD, lanes), b16),
            pltpu.VMEM((pairs, HEAD, lanes), b16),
            dma((2,)),
            dma((2, pairs)),
            dma((2, pairs)),
            dma((pairs,)),
            dma((pairs,)),
            dma((pairs,)),
        ],
        compiler_params=pltpu.CompilerParams(collective_id=1, has_side_effects=True),
    )(
        queries,
        keys,
        values,
        decays,
        rates,
        surges,
        documents.reshape(1, rows),
        scale.reshape(1, width),
    )


def tp_reduce_kernel(size, groups, sends_back, *refs):
    if sends_back:
        (parts, extra, out, extra_out, near, pair, far, enear, epair, efar, stage) = refs[:11]
        sems = refs[11:]
    else:
        (parts, out, near, pair, far) = refs[:5]
        sems = refs[5:]
    nsend, nrecv, fsend, frecv = sems[:4]
    me = lax.axis_index("tp")
    own = lax.axis_index("sp")
    half = size // 2
    partner = me + 1 - 2 * lax.rem(me, 2)
    pieces = parts.shape[1]
    greet((("tp", size), ("sp", groups)) if sends_back else (("tp", size),))

    jobs = []
    for step in range(pieces):
        where = lax.rem(own + 1 + step, pieces) if sends_back else step
        jobs.append((step, parts, near, pair, far, where))
    if sends_back:
        jobs.append((pieces, extra, enear, epair, efar, 0))

    def near_copy(job, k):
        slot, src, to, _, _, where = job
        return remote(
            src.at[lax.rem(partner + 2 * k, size), where],
            to.at[k, where],
            nsend.at[slot, k],
            nrecv.at[slot, k],
            "tp",
            partner,
        )

    def far_copy(job, k):
        slot, _, _, src, to, where = job
        return remote(
            src.at[k - 1, where],
            to.at[k - 1, where],
            fsend.at[slot, k],
            frecv.at[slot, k],
            "tp",
            lax.rem(me + 2 * k, size),
        )

    for job in jobs:
        for k in range(half - 1, -1, -1):
            near_copy(job, k).start()

    def add_pair(job):
        slot, src, to, mid, _, where = job
        for k in range(1, half):
            near_copy(job, k).wait_recv()
            mid[k - 1, where] = (
                src[lax.rem(me + 2 * k, size), where].astype(jnp.float32)
                + to[k, where].astype(jnp.float32)
            ).astype(jnp.bfloat16)
            far_copy(job, k).start()

    def back_copy(step):
        target = lax.rem(own + 1 + step, pieces)
        return remote(
            stage.at[target], out.at[own], sems[4].at[step], sems[5].at[step], "sp", target
        )

    def finish(job):
        slot, src, to, _, last, where = job
        near_copy(job, 0).wait_recv()
        total = src[me, where].astype(jnp.float32) + to[0, where].astype(jnp.float32)
        for k in range(1, half):
            far_copy(job, k).wait_recv()
            total = total + last[k - 1, where].astype(jnp.float32)
        if not sends_back:
            out[where] = total
        elif slot == pieces:
            extra_out[...] = total
        elif slot == pieces - 1:
            out[own] = total.astype(jnp.bfloat16)
        else:
            stage[where] = total.astype(jnp.bfloat16)
            back_copy(slot).start()

    lag = 2
    for turn in range(len(jobs) + lag):
        if turn < len(jobs):
            add_pair(jobs[turn])
        if turn >= lag:
            finish(jobs[turn - lag])
    for job in jobs:
        for k in range(half):
            near_copy(job, k).wait_send()
        for k in range(1, half):
            far_copy(job, k).wait_send()
    if sends_back:
        for step in range(pieces - 1):
            back_copy(step).wait_send()
            sender = lax.rem(own - 1 - step + pieces, pieces)
            remote(
                stage.at[sender], out.at[sender], sems[4].at[step], sems[5].at[step], "sp", sender
            ).wait_recv()


def tp_reduce(parts):
    size, pieces, rows, width = parts.shape
    half = size // 2
    kind = jnp.bfloat16
    return pl.pallas_call(
        lambda *refs: tp_reduce_kernel(size, 1, False, *refs),
        out_shape=jax.ShapeDtypeStruct((pieces, rows, width), jnp.float32),
        in_specs=[VMEM],
        out_specs=VMEM,
        scratch_shapes=[
            pltpu.VMEM((half, pieces, rows, width), kind),
            pltpu.VMEM((half - 1, pieces, rows, width), kind),
            pltpu.VMEM((half - 1, pieces, rows, width), kind),
        ]
        + [pltpu.SemaphoreType.DMA((pieces, half))] * 4,
        compiler_params=pltpu.CompilerParams(collective_id=2, has_side_effects=True),
    )(parts)


def tp_reduce_return(parts, extra):
    size, pieces, rows, width = parts.shape
    more = extra.shape[1]
    half = size // 2
    kind = jnp.bfloat16
    return pl.pallas_call(
        lambda parts_ref, extra_ref, *refs: tp_reduce_kernel(
            size, pieces, True, parts_ref, extra_ref, *refs
        ),
        out_shape=(
            jax.ShapeDtypeStruct((pieces, rows, width), kind),
            jax.ShapeDtypeStruct((more, width), jnp.float32),
        ),
        in_specs=[VMEM, VMEM],
        out_specs=(VMEM, VMEM),
        scratch_shapes=[
            pltpu.VMEM((half, pieces, rows, width), kind),
            pltpu.VMEM((half - 1, pieces, rows, width), kind),
            pltpu.VMEM((half - 1, pieces, rows, width), kind),
            pltpu.VMEM((half, 1, more, width), kind),
            pltpu.VMEM((half - 1, 1, more, width), kind),
            pltpu.VMEM((half - 1, 1, more, width), kind),
            pltpu.VMEM((pieces, rows, width), kind),
        ]
        + [pltpu.SemaphoreType.DMA((pieces + 1, half))] * 4
        + [pltpu.SemaphoreType.DMA((pieces,))] * 2,
        compiler_params=pltpu.CompilerParams(
            collective_id=3, has_side_effects=True, vmem_limit_bytes=60 * 1024 * 1024
        ),
    )(parts, extra[:, None])


def dispatch_kernel(
    size, groups, outgoing, stream, arrived, rows_all, local, asend, arecv, nsend, nrecv, fsend, frecv, gsend, grecv
):
    me = lax.axis_index("tp")
    own = lax.axis_index("sp")
    half = size // 2
    partner = me + 1 - 2 * lax.rem(me, 2)
    greet((("tp", size), ("sp", groups)))

    def exchange(step):
        return remote(
            outgoing.at[lax.rem(own + step, groups)],
            arrived.at[me, own],
            asend.at[step],
            arecv.at[step],
            "sp",
            lax.rem(own + step, groups),
        )

    def place(step, who):
        if step == groups:
            return rows_all.at[who]
        return arrived.at[who, lax.rem(own - step + groups, groups)]

    def source(step):
        if step == groups:
            return stream
        return outgoing.at[own] if step == 0 else place(step, me)

    def near_copy(step):
        return remote(source(step), place(step, me), nsend.at[step], nrecv.at[step], "tp", partner)

    def far_copy(step, k):
        return remote(
            source(step),
            place(step, me),
            fsend.at[step, k],
            frecv.at[step, k],
            "tp",
            lax.rem(me + 2 * k, size),
        )

    def forward(step, k):
        who = place(step, lax.rem(me - 2 * k + size, size))
        return remote(who, who, gsend.at[step, k], grecv.at[step, k], "tp", partner)

    def start_own(step):
        for k in range(1, half):
            far_copy(step, k).start()
        near_copy(step).start()

    def pass_on(step):
        for k in range(1, half):
            far_copy(step, k).wait_recv()
            forward(step, k).start()

    keep_block = pltpu.make_async_copy(outgoing.at[own], arrived.at[me, own], local.at[0])
    keep_rows = pltpu.make_async_copy(stream, rows_all.at[me], local.at[1])
    for step in range(1, groups):
        exchange(step).start()
    keep_block.start()
    keep_rows.start()
    order = [groups] + list(range(groups))
    for turn, step in enumerate(order):
        if 0 < step < groups:
            exchange(step).wait_recv()
        start_own(step)
        if turn > 0:
            pass_on(order[turn - 1])
    pass_on(order[-1])
    keep_block.wait()
    keep_rows.wait()
    for step in range(1, groups):
        exchange(step).wait_send()
    for step in order:
        near_copy(step).wait()
        for k in range(1, half):
            far_copy(step, k).wait_send()
            forward(step, k).wait()


def dispatch(outgoing, stream):
    size = lax.axis_size("tp")
    groups, rows, width = outgoing.shape
    half = size // 2
    dma = pltpu.SemaphoreType.DMA
    return pl.pallas_call(
        lambda *refs: dispatch_kernel(size, groups, *refs),
        out_shape=(
            jax.ShapeDtypeStruct((size, groups, rows, width), jnp.bfloat16),
            jax.ShapeDtypeStruct((size,) + stream.shape, jnp.bfloat16),
        ),
        in_specs=[VMEM, VMEM],
        out_specs=(VMEM, VMEM),
        scratch_shapes=[dma((2,)), dma((groups,)), dma((groups,))]
        + [dma((groups + 1,))] * 2
        + [dma((groups + 1, half))] * 4,
        compiler_params=pltpu.CompilerParams(collective_id=4, has_side_effects=True),
    )(outgoing, stream)


def per_device(
    head_queries,
    head_keys,
    head_values,
    decay_logits,
    learning_logits,
    surge_decay,
    documents,
    residual,
    head_norm_scale,
    mixer_output_weight,
    layer_norm_scale,
    routes,
    routing_weight,
    routed_gate_weight,
    routed_up_weight,
    routed_down_weight,
    common_gate_weight,
    common_up_weight,
    common_down_weight,
):
    head_outputs = mixer(
        head_queries,
        head_keys,
        head_values,
        decay_logits,
        learning_logits,
        surge_decay,
        documents,
        head_norm_scale,
    )
    quarters = lax.axis_size("tp")
    groups = lax.axis_size("sp")
    own_rows, model_width = residual.shape
    pieces = own_rows // 16
    mixed_parts = jnp.dot(
        head_outputs, mixer_output_weight, preferred_element_type=jnp.float32
    ).astype(jnp.bfloat16)
    mixed_rows = tp_reduce(mixed_parts.reshape(quarters, pieces, 16, model_width)).reshape(
        own_rows, model_width
    )
    summed = residual_scale * residual.astype(jnp.float32) + mixed_rows
    centre = jnp.mean(summed, -1, keepdims=True)
    spread = jnp.mean(jnp.square(summed - centre), -1, keepdims=True)
    stream = ((summed - centre) * lax.rsqrt(spread + norm_eps) * layer_norm_scale).astype(
        jnp.bfloat16
    )
    experts = EXP_DEV * groups
    capacity = max(2, (3 * TOK_DEV * TOP + 2 * experts - 1) // (2 * experts))
    chosen = routes.reshape(quarters, own_rows * TOP)
    onehot = (chosen[..., None] == jnp.arange(experts, dtype=jnp.int32)).astype(jnp.int32)
    ranking = jnp.sum(jnp.cumsum(onehot, 1) * onehot, -1) - 1
    slot_index = chosen * capacity + ranking
    own_slots = lax.dynamic_index_in_dim(slot_index, lax.axis_index("tp"), 0, keepdims=False)
    own_slots = own_slots.reshape(own_rows, TOP)
    slots = jnp.arange(experts * capacity, dtype=jnp.int32)
    hits = own_slots[:, :, None] == slots
    spread_to = jnp.any(hits, 1).astype(jnp.bfloat16)
    block_rows = EXP_DEV * capacity
    outgoing = jnp.einsum(
        "ts,td->sd", spread_to, stream, preferred_element_type=jnp.float32
    ).astype(jnp.bfloat16)
    arrived_all, rows_all = dispatch(outgoing.reshape(groups, block_rows, model_width), stream)
    rows_in = arrived_all.reshape(quarters * groups * block_rows, model_width)
    hosted = (jnp.arange(rows_in.shape[0], dtype=jnp.int32) % block_rows) // capacity
    hidden_list = []
    for expert in range(EXP_DEV):
        gated = jnp.dot(rows_in, routed_gate_weight[expert], preferred_element_type=jnp.float32)
        lifted = jnp.dot(rows_in, routed_up_weight[expert], preferred_element_type=jnp.float32)
        hidden = (jax.nn.silu(gated) * lifted).astype(jnp.bfloat16)
        hidden_list.append(
            jnp.where((hosted == expert)[:, None], hidden, jnp.zeros_like(hidden))
        )
    partial_value = jnp.dot(
        jnp.concatenate(hidden_list, -1),
        routed_down_weight.reshape(-1, model_width),
        preferred_element_type=jnp.float32,
    ).astype(jnp.bfloat16)
    rows_all = rows_all.reshape(quarters * own_rows, model_width)
    shared_gated = jnp.dot(rows_all, common_gate_weight, preferred_element_type=jnp.float32)
    shared_lifted = jnp.dot(rows_all, common_up_weight, preferred_element_type=jnp.float32)
    shared_hidden = (jax.nn.silu(shared_gated) * shared_lifted).astype(jnp.bfloat16)
    shared_part = jnp.dot(
        shared_hidden, common_down_weight, preferred_element_type=jnp.float32
    ).astype(jnp.bfloat16)
    returned, shared_sum = tp_reduce_return(
        partial_value.reshape(quarters, groups, block_rows, model_width),
        shared_part.reshape(quarters, own_rows, model_width),
    )
    weights = jnp.sum(jnp.where(hits, routing_weight[:, :, None], 0.0), 1)
    routed = jnp.dot(
        weights,
        returned.reshape(experts * capacity, model_width).astype(jnp.float32),
        precision=lax.Precision.HIGHEST,
    )
    return (residual_scale * stream.astype(jnp.float32) + routed + shared_sum).astype(jnp.bfloat16)


def solution(mesh):
    placed = (
        P("sp", "tp"),
        P("sp", "tp"),
        P("sp", "tp"),
        P("sp", "tp"),
        P("sp", "tp"),
        P("sp", "tp"),
        P("sp"),
        P(("sp", "tp"), None),
        P("tp"),
        P("tp", None),
        P(),
        P("sp", None),
        P(("sp", "tp"), None),
        P("sp", None, "tp"),
        P("sp", None, "tp"),
        P("sp", "tp", None),
        P(None, "tp"),
        P(None, "tp"),
        P("tp", None),
    )
    return jax.shard_map(
        per_device, mesh=mesh, in_specs=placed, out_specs=P(("sp", "tp"), None), check_vma=False
    )
```

```python
import jax
import jax.numpy as jnp
from jax import lax
from jax.experimental import pallas as pl
from jax.experimental.pallas import tpu as pltpu
from jax.sharding import PartitionSpec as P

HEAD = 64
EXP_DEV = 2
TOP = 2
BLOCK_SPAN = 64
TOK_DEV = 64


residual_scale = 2.0**0.5
group_eps = 0.00064
norm_eps = 1e-05
unit_eps = 1e-06
CLOSE = 2
EXTRA_TURN = 5
SCORE_PRECISION = lax.Precision.HIGH


MESH = pl.DeviceIdType.MESH
VMEM = pl.BlockSpec(memory_space=pltpu.VMEM)


def remote(src, dst, send_sem, recv_sem, axis, index):
    return pltpu.make_async_remote_copy(
        src_ref=src,
        dst_ref=dst,
        send_sem=send_sem,
        recv_sem=recv_sem,
        device_id={axis: index},
        device_id_type=MESH,
    )


def greet(groups):
    barrier = pltpu.get_barrier_semaphore()
    count = 0
    for axis, size in groups:
        me = lax.axis_index(axis)
        for step in range(1, size):
            pl.semaphore_signal(
                barrier,
                inc=1,
                device_id={axis: lax.rem(me + step, size)},
                device_id_type=MESH,
            )
            count += 1
    pl.semaphore_wait(barrier, count)


def chunk_iota(rows, cols, dim):
    return lax.broadcasted_iota(jnp.int32, (rows, cols), dim)


def mm(left, right, precision=None):
    return jnp.dot(left, right, preferred_element_type=jnp.float32, precision=precision)


def mm_nt(left, right, precision=None):
    return lax.dot_general(
        left,
        right,
        (((1,), (1,)), ((), ())),
        preferred_element_type=jnp.float32,
        precision=precision,
    )


def mm_tn(left, right, precision=None):
    return lax.dot_general(
        left,
        right,
        (((0,), (0,)), ((), ())),
        preferred_element_type=jnp.float32,
        precision=precision,
    )


def narrow(values):
    return values.astype(jnp.bfloat16)


def split(values):
    top = narrow(values)
    return top, narrow(values - top.astype(jnp.float32))


def mixer_kernel(
    size,
    queries,
    keys,
    values,
    decays,
    rates,
    surges,
    docs,
    scale,
    out,
    unit_s,
    ahead_s,
    fwd_s,
    reads_s,
    solved_s,
    map_s,
    add_s,
    local_s,
    starts_s,
    comp_s,
    far_s,
    join_s,
    doc_out,
    doc_in,
    padd_out,
    padd_in,
    pmap_out,
    pmap_in,
    s_out,
    s_in,
    doc_sem,
    padd_sem,
    pmap_sem,
    near_sem,
    next_sem,
    s_recv,
):
    me = lax.axis_index("sp")
    span = BLOCK_SPAN
    rows, width = queries.shape
    chunks = rows // span
    lanes = 2 * HEAD
    pairs = width // lanes
    heads = rates.shape[1]
    high = lax.Precision.HIGH
    barrier = pltpu.get_barrier_semaphore()
    for step in (1, 2, size - 1, size - 2):
        pl.semaphore_signal(
            barrier, inc=1, device_id={"sp": lax.rem(me + step, size)}, device_id_type=MESH
        )

    same_half = (chunk_iota(lanes, lanes, 0) // HEAD) == (chunk_iota(lanes, lanes, 1) // HEAD)
    ones_half = same_half.astype(jnp.float32)
    earlier = lax.rem(chunk_iota(span, lanes, 1), HEAD)
    later = chunk_iota(span, lanes, 0)
    unit_pair = (earlier == later).astype(jnp.float32)
    unit_full = (chunk_iota(lanes, lanes, 0) == chunk_iota(lanes, lanes, 1)).astype(jnp.float32)

    def wide(block):
        return jnp.where(same_half, jnp.concatenate([block, block], 0), 0.0)

    row_docs = docs[...].astype(jnp.float32)
    row_square = jnp.broadcast_to(row_docs, (rows, rows))
    diag = chunk_iota(rows, rows, 0) == chunk_iota(rows, rows, 1)
    doc_col = mm(
        narrow(jnp.where(diag, row_square, 0.0)), jnp.ones((rows, lanes), jnp.bfloat16)
    )
    pick = (
        lax.rem(chunk_iota(rows, lanes, 0), span) == lax.rem(chunk_iota(rows, lanes, 1), HEAD)
    ).astype(jnp.bfloat16)
    wide_rows = 8 * ((chunks + 7) // 8)
    in_chunk = (chunk_iota(wide_rows, rows, 1) // span) == chunk_iota(wide_rows, rows, 0)
    doc_row = mm(
        narrow(jnp.where(in_chunk, jnp.broadcast_to(row_docs, (wide_rows, rows)), 0.0)), pick
    )
    same_chunk = (chunk_iota(rows, rows, 0) // span) == (chunk_iota(rows, rows, 1) // span)
    tri = (
        (chunk_iota(rows, rows, 0) >= chunk_iota(rows, rows, 1)) & same_chunk
    ).astype(jnp.bfloat16)

    strict, causal, joined, tail = [], [], [], []
    for c in range(chunks):
        col = doc_col[c * span : (c + 1) * span]
        same_doc = col == doc_row[c : c + 1]
        strict.append(same_doc & (later > earlier))
        causal.append(same_doc & (later >= earlier))
        before_row = doc_col[max(c * span - 1, 0) : max(c * span - 1, 0) + 1]
        joined.append((col == before_row).astype(jnp.float32))
        tail.append((col == doc_col[(c + 1) * span - 1 : (c + 1) * span]).astype(jnp.float32))

    doc_out[...] = jnp.broadcast_to(doc_col[rows - 1 : rows], doc_out.shape)
    pl.semaphore_wait(barrier, 4)
    following = lax.rem(me + 1, size)
    doc_hop = remote(doc_out, doc_in, doc_sem.at[0], doc_sem.at[1], "sp", following)

    @pl.when(me < size - 1)
    def _():
        doc_hop.start()

    rate_all = jax.nn.sigmoid(rates[...].astype(jnp.float32))
    surge_all = surges[...]

    def local_pairs(turn, carry):
        streams = []
        for half in range(2):
            p = turn * 2 + half
            cols = pl.ds(pl.multiple_of(p * lanes, lanes), lanes)
            spread_heads = (
                chunk_iota(heads, lanes, 0) == 2 * p + chunk_iota(heads, lanes, 1) // HEAD
            ).astype(jnp.float32)
            key = keys[:, cols].astype(jnp.float32)
            norm = mm(key * key, ones_half, high)
            unit = key * lax.rsqrt(norm + unit_eps)
            rate = mm(rate_all, spread_heads, high)
            surge = mm(surge_all, spread_heads, high)
            logit = decays[:, cols].astype(jnp.float32)
            decay = surge - jnp.exp(-0.5) / (1.0 + jnp.exp(-logit))
            top, rest = split(decay)
            cumulative = mm(tri, top) + mm(tri, rest)
            grown = jnp.exp(cumulative)
            shrunk = jnp.exp(-cumulative)
            ahead = unit * jnp.exp(cumulative - decay)
            unit_rate = unit * rate
            back_unit = unit_rate * shrunk
            back_key = key * shrunk
            forward = queries[:, cols].astype(jnp.float32) * grown
            ahead_s[:, cols] = ahead
            fwd_s[:, cols] = forward
            for c in range(chunks):
                part = slice(c * span, (c + 1) * span)
                total = cumulative[(c + 1) * span - 1 : (c + 1) * span]
                ending = jnp.exp(total - cumulative[part]) * tail[c]
                streams.append(
                    dict(
                        c=c,
                        p=p,
                        cols=cols,
                        ahead=ahead[part],
                        fwd=forward[part],
                        bu=back_unit[part],
                        bk=back_key[part],
                        eu=-unit_rate[part] * ending,
                        ek=key[part] * ending,
                        val=values[part, cols].astype(jnp.float32),
                        keep=jnp.exp(total) * joined[c][span - 1 : span],
                    )
                )
        for s in streams:
            c = s["c"]
            scores = mm_nt(
                jnp.concatenate([s["ahead"], s["fwd"]], 0),
                jnp.concatenate([wide(s["bu"]), wide(s["bk"])], 0),
                SCORE_PRECISION,
            )
            s["low"] = jnp.where(strict[c], scores[:span, :lanes], 0.0)
            s["mixk"] = jnp.where(strict[c], scores[:span, lanes:], 0.0)
            reads_s[c, s["p"], :, :lanes] = narrow(
                jnp.where(causal[c], -scores[span:, :lanes], 0.0)
            )
            reads_s[c, s["p"], :, lanes:] = narrow(jnp.where(causal[c], scores[span:, lanes:], 0.0))
        base = 16
        near_block = (earlier // base) == (later // base)
        for s in streams:
            s["low_near"] = jnp.where(near_block, s["low"], 0.0)
            s["inv"] = unit_pair - s["low_near"]
        for s in streams:
            s["power"] = mm(s["low_near"], wide(s["low_near"]), high)
            s["mv"] = mm(s["mixk"], wide(s["val"]))
        reach = 2
        while reach < base:
            last = reach * 2 >= base
            for s in streams:
                right = wide(s["power"])
                if last:
                    s["inv"] = s["inv"] + mm(s["inv"], right, high)
                else:
                    both = mm(jnp.concatenate([s["power"], s["inv"]], 0), right, high)
                    s["power"] = both[:span]
                    s["inv"] = s["inv"] + both[span:]
            reach = reach * 2
        while base < span:
            off = ((earlier // base) != (later // base)) & (
                (earlier // (2 * base)) == (later // (2 * base))
            )
            for s in streams:
                s["mid"] = mm(s["inv"], wide(jnp.where(off, s["low"], 0.0)), high)
            for s in streams:
                s["inv"] = s["inv"] - mm(s["mid"], wide(s["inv"]), high)
            base = base * 2
        for s in streams:
            c = s["c"]
            s["solved"] = mm(
                s["inv"],
                jnp.concatenate([wide(s["ahead"] * joined[c]), wide(s["mv"])], 1),
                high,
            )
            solved_s[c, s["p"]] = narrow(s["solved"])
        for s in streams:
            c, p = s["c"], s["p"]
            pull = mm_tn(s["solved"][:, :lanes], s["eu"], high)
            map_s[c, p] = jnp.where(same_half, pull, 0.0) + unit_full * s["keep"]
            grown = mm_tn(
                jnp.concatenate([s["solved"][:, lanes:], s["val"]], 0),
                jnp.concatenate([s["eu"], s["ek"]], 0),
                high,
            )
            grown = jnp.where(same_half, grown, 0.0)
            add_s[c, p] = grown[:HEAD] + grown[HEAD:]
        return carry

    lax.fori_loop(0, pairs // 2, local_pairs, 0)

    state = [None] * pairs
    for p in range(pairs):
        state[p] = jnp.concatenate([add_s[0, p], map_s[0, p][:HEAD] + map_s[0, p][HEAD:]], 0)
    kept = [state]
    for c in range(1, chunks):
        state = [
            mm(kept[-1][p], map_s[c, p], high)
            + jnp.concatenate([add_s[c, p], jnp.zeros((HEAD, lanes), jnp.float32)], 0)
            for p in range(pairs)
        ]
        kept.append(state)
    finals = kept[-1]

    @pl.when(me == 0)
    def _():
        join_s[...] = jnp.zeros_like(join_s)
        s_in[...] = jnp.zeros_like(s_in)

    @pl.when(me > 0)
    def _():
        doc_hop.wait_recv()
        join_s[...] = (doc_in[...] == doc_col[0:1]).astype(jnp.float32)

    join = join_s[0:1]
    for p in range(pairs):
        comp_s[p] = jnp.concatenate([finals[p][:HEAD], finals[p][HEAD:] * join], 0)
    even = lax.rem(me, 2) == 0

    def pair_hop(p):
        return (
            remote(padd_out.at[p], padd_in.at[p], padd_sem.at[0, p], padd_sem.at[1, p], "sp", following),
            remote(pmap_out.at[p], pmap_in.at[p], pmap_sem.at[0, p], pmap_sem.at[1, p], "sp", following),
        )

    def state_hop(p, near):
        sem = near_sem if near else next_sem
        return remote(
            s_out.at[p],
            s_in.at[p],
            sem.at[p],
            s_recv.at[p],
            "sp",
            lax.rem(me + (2 if near else 1), size),
        )

    @pl.when(even)
    def _():
        for p in range(pairs):
            padd_out[p] = narrow(comp_s[p, :HEAD])
            pmap_out[p] = comp_s[p, HEAD:]
        for p in range(pairs):
            pair_hop(p)[0].start()
        for p in range(pairs):
            pair_hop(p)[1].start()

    def finish_local():
        for p in range(pairs):
            cols = slice(p * lanes, (p + 1) * lanes)
            for c in range(chunks):
                part = slice(c * span, (c + 1) * span)
                read_unit = reads_s[c, p, :, :lanes]
                solved = solved_s[c, p].astype(jnp.float32)
                local = mm(
                    reads_s[c, p],
                    jnp.concatenate(
                        [
                            narrow(wide(solved[:, lanes:])),
                            narrow(wide(values[part, cols].astype(jnp.float32))),
                        ],
                        0,
                    ),
                )
                start = fwd_s[part, cols] * joined[c] + mm(
                    read_unit, narrow(wide(solved[:, :lanes]))
                )
                if c > 0:
                    seen = mm_nt(
                        narrow(start),
                        jnp.concatenate(
                            [
                                narrow(wide(kept[c - 1][p][:HEAD])),
                                narrow(wide(kept[c - 1][p][HEAD:])),
                            ],
                            0,
                        ),
                    )
                    local = local + seen[:, :lanes]
                    start = seen[:, lanes:]
                local_s[part, cols] = local
                starts_s[part, cols] = narrow(start)

    finish_local()

    @pl.when(jnp.logical_not(even))
    def _():
        for p in range(pairs):
            pair_hop(p)[0].wait_recv()
            first = padd_in[p]
            top, rest = split(wide(comp_s[p, HEAD:]))
            far_s[p, :HEAD] = (
                mm(jnp.concatenate([first, first], 1), jnp.concatenate([top, rest], 0))
                + comp_s[p, :HEAD]
            )

        @pl.when(me == 1)
        def _():
            s_in[...] = jnp.zeros_like(s_in)
            for p in range(pairs):
                s_out[p] = narrow(far_s[p, :HEAD])
                state_hop(p, True).start()

        for p in range(pairs):
            pair_hop(p)[1].wait_recv()

        @pl.when(me > 1)
        def _():
            for p in range(pairs):
                both = mm(pmap_in[p], wide(comp_s[p, HEAD:]), high)
                far_s[p, HEAD:] = both
            weights = []
            for p in range(pairs):
                top, rest = split(wide(far_s[p, HEAD:]))
                weights.append(jnp.concatenate([top, rest], 0))
            for p in range(pairs):
                state_hop(p, True).wait_recv()

                @pl.when(me < size - 1)
                def _():
                    arrived = s_in[p]
                    s_out[p] = narrow(
                        mm(jnp.concatenate([arrived, arrived], 1), weights[p]) + far_s[p, :HEAD]
                    )
                    state_hop(p, True).start()

        @pl.when(me < size - 1)
        def _():
            for p in range(pairs):
                state_hop(p, False).start()

        for p in range(pairs):
            top, rest = split(wide(pmap_in[p]))
            arrived = s_in[p]
            comp_s[p, :HEAD] = (
                mm(jnp.concatenate([arrived, arrived], 1), jnp.concatenate([top, rest], 0))
                + padd_in[p].astype(jnp.float32)
            )

    @pl.when(even)
    def _():
        @pl.when(me > 0)
        def _():
            for p in range(pairs):
                state_hop(p, False).wait_recv()

        for p in range(pairs):
            comp_s[p, :HEAD] = s_in[p].astype(jnp.float32)

    for p in range(pairs):
        cols = slice(p * lanes, (p + 1) * lanes)
        incoming = narrow(wide(comp_s[p, :HEAD] * join))
        read = local_s[:, cols] + mm_nt(starts_s[:, cols], incoming)
        centred = read - mm(read, ones_half, high) * (1.0 / HEAD)
        spread = mm(centred * centred, ones_half, high) * (1.0 / HEAD)
        out[:, cols] = narrow(centred * lax.rsqrt(spread + group_eps) * scale[:, cols])

    @pl.when(me < size - 1)
    def _():
        doc_hop.wait_send()

    @pl.when(even)
    def _():
        for p in range(pairs):
            for hop in pair_hop(p):
                hop.wait_send()

    @pl.when(jnp.logical_not(even) & (me < size - 1))
    def _():
        for p in range(pairs):
            state_hop(p, True).wait_send()
            state_hop(p, False).wait_send()


def mixer(queries, keys, values, decays, rates, surges, documents, scale):
    size = lax.axis_size("sp")
    rows, width = queries.shape
    lanes = 2 * HEAD
    pairs = width // lanes
    chunks = rows // BLOCK_SPAN
    f32, b16 = jnp.float32, jnp.bfloat16
    dma = pltpu.SemaphoreType.DMA
    return pl.pallas_call(
        lambda *refs: mixer_kernel(size, *refs),
        out_shape=jax.ShapeDtypeStruct((rows, width), b16),
        in_specs=[VMEM] * 8,
        out_specs=VMEM,
        scratch_shapes=[
            pltpu.VMEM((8, lanes), f32),
            pltpu.VMEM((rows, width), f32),
            pltpu.VMEM((rows, width), f32),
            pltpu.VMEM((chunks, pairs, BLOCK_SPAN, 2 * lanes), b16),
            pltpu.VMEM((chunks, pairs, BLOCK_SPAN, 2 * lanes), b16),
            pltpu.VMEM((chunks, pairs, lanes, lanes), f32),
            pltpu.VMEM((chunks, pairs, HEAD, lanes), f32),
            pltpu.VMEM((rows, width), f32),
            pltpu.VMEM((rows, width), b16),
            pltpu.VMEM((pairs, lanes, lanes), f32),
            pltpu.VMEM((pairs, lanes, lanes), f32),
            pltpu.VMEM((8, lanes), f32),
            pltpu.VMEM((8, lanes), f32),
            pltpu.VMEM((8, lanes), f32),
            pltpu.VMEM((pairs, HEAD, lanes), b16),
            pltpu.VMEM((pairs, HEAD, lanes), b16),
            pltpu.VMEM((pairs, HEAD, lanes), f32),
            pltpu.VMEM((pairs, HEAD, lanes), f32),
            pltpu.VMEM((pairs, HEAD, lanes), b16),
            pltpu.VMEM((pairs, HEAD, lanes), b16),
            dma((2,)),
            dma((2, pairs)),
            dma((2, pairs)),
            dma((pairs,)),
            dma((pairs,)),
            dma((pairs,)),
        ],
        compiler_params=pltpu.CompilerParams(collective_id=1, has_side_effects=True),
    )(
        queries,
        keys,
        values,
        decays,
        rates,
        surges,
        documents.reshape(1, rows),
        scale.reshape(1, width),
    )


def tp_reduce_kernel(size, groups, sends_back, *refs):
    if sends_back:
        (parts, extra, out, extra_out, near, pair, far, enear, epair, efar, stage) = refs[:11]
        sems = refs[11:]
    else:
        (parts, out, near, pair, far) = refs[:5]
        sems = refs[5:]
    nsend, nrecv, fsend, frecv = sems[:4]
    me = lax.axis_index("tp")
    own = lax.axis_index("sp")
    half = size // 2
    partner = me + 1 - 2 * lax.rem(me, 2)
    pieces = parts.shape[1]
    greet((("tp", size), ("sp", groups)) if sends_back else (("tp", size),))

    jobs = []
    for step in range(pieces):
        where = lax.rem(own + 1 + step, pieces) if sends_back else step
        jobs.append((step, parts, near, pair, far, where))
    if sends_back:
        jobs.append((pieces, extra, enear, epair, efar, 0))

    def near_copy(job, k):
        slot, src, to, _, _, where = job
        return remote(
            src.at[lax.rem(partner + 2 * k, size), where],
            to.at[k, where],
            nsend.at[slot, k],
            nrecv.at[slot, k],
            "tp",
            partner,
        )

    def far_copy(job, k):
        slot, _, _, src, to, where = job
        return remote(
            src.at[k - 1, where],
            to.at[k - 1, where],
            fsend.at[slot, k],
            frecv.at[slot, k],
            "tp",
            lax.rem(me + 2 * k, size),
        )

    for job in jobs:
        for k in range(half - 1, -1, -1):
            near_copy(job, k).start()

    def add_pair(job):
        slot, src, to, mid, _, where = job
        for k in range(1, half):
            near_copy(job, k).wait_recv()
            mid[k - 1, where] = (
                src[lax.rem(me + 2 * k, size), where].astype(jnp.float32)
                + to[k, where].astype(jnp.float32)
            ).astype(jnp.bfloat16)
            far_copy(job, k).start()

    def back_copy(step):
        target = lax.rem(own + 1 + step, pieces)
        return remote(
            stage.at[target], out.at[own], sems[4].at[step], sems[5].at[step], "sp", target
        )

    def finish(job):
        slot, src, to, _, last, where = job
        near_copy(job, 0).wait_recv()
        total = src[me, where].astype(jnp.float32) + to[0, where].astype(jnp.float32)
        for k in range(1, half):
            far_copy(job, k).wait_recv()
            total = total + last[k - 1, where].astype(jnp.float32)
        if not sends_back:
            out[where] = total
        elif slot == pieces:
            extra_out[...] = total
        elif slot == pieces - 1:
            out[own] = total.astype(jnp.bfloat16)
        else:
            stage[where] = total.astype(jnp.bfloat16)
            back_copy(slot).start()

    lag = 2
    for turn in range(len(jobs) + lag):
        if turn < len(jobs):
            add_pair(jobs[turn])
        if turn >= lag:
            finish(jobs[turn - lag])
    for job in jobs:
        for k in range(half):
            near_copy(job, k).wait_send()
        for k in range(1, half):
            far_copy(job, k).wait_send()
    if sends_back:
        for step in range(pieces - 1):
            back_copy(step).wait_send()
            sender = lax.rem(own - 1 - step + pieces, pieces)
            remote(
                stage.at[sender], out.at[sender], sems[4].at[step], sems[5].at[step], "sp", sender
            ).wait_recv()


def tp_reduce(parts):
    size, pieces, rows, width = parts.shape
    half = size // 2
    kind = jnp.bfloat16
    return pl.pallas_call(
        lambda *refs: tp_reduce_kernel(size, 1, False, *refs),
        out_shape=jax.ShapeDtypeStruct((pieces, rows, width), jnp.float32),
        in_specs=[VMEM],
        out_specs=VMEM,
        scratch_shapes=[
            pltpu.VMEM((half, pieces, rows, width), kind),
            pltpu.VMEM((half - 1, pieces, rows, width), kind),
            pltpu.VMEM((half - 1, pieces, rows, width), kind),
        ]
        + [pltpu.SemaphoreType.DMA((pieces, half))] * 4,
        compiler_params=pltpu.CompilerParams(collective_id=2, has_side_effects=True),
    )(parts)


def flip(index, bits, size):
    total = 0
    place = 1
    while place < size:
        total = total + lax.rem(lax.div(index, place) + lax.div(bits, place), 2) * place
        place = place * 2
    return total


def moe_kernel(
    size,
    groups,
    capacity,
    block,
    choice,
    stream,
    mix,
    gate,
    upward,
    down,
    common_gate,
    common_up,
    common_down,
    out,
    outgoing,
    near_out,
    mix_far,
    returned_far,
    stage_far,
    arrived,
    rows_all,
    parts,
    near,
    pair,
    far,
    stage,
    returned,
    extra,
    enear,
    epair,
    efar,
    gate_v,
    up_v,
    down_v,
    cgate_v,
    cup_v,
    cdown_v,
    local,
    loads,
    asend,
    arecv,
    nsend,
    nrecv,
    fsend,
    frecv,
    gsend,
    grecv,
    rnsend,
    rnrecv,
    rfsend,
    rfrecv,
    bsend,
    brecv,
    msend,
    mrecv,
):
    me = lax.axis_index("tp")
    own = lax.axis_index("sp")
    half = size // 2
    partner = me + 1 - 2 * lax.rem(me, 2)
    tokens, width = stream.shape
    close = min(CLOSE, groups)
    batch = max(1, groups // 8)
    steps = groups // batch
    fetches = [
        pltpu.make_async_copy(src, dst, loads.at[i])
        for i, (src, dst) in enumerate(
            (
                (common_gate, cgate_v),
                (common_up, cup_v),
                (common_down, cdown_v),
                (gate, gate_v),
                (upward, up_v),
                (down, down_v),
            )
        )
    ]
    for fetch in fetches:
        fetch.start()
    keep_rows = pltpu.make_async_copy(stream, rows_all.at[me], local.at[1])
    keep_rows.start()
    returned_far[...] = jnp.zeros_like(returned_far)
    outgoing[...] = narrow(mm(narrow(choice[me]), stream[...])).reshape(groups, block, width)
    greet((("tp", size), ("sp", groups)))

    def ahead(j):
        return lax.rem(me + 2 * j, size)

    def exchange(k, j=0, near=False):
        other = flip(own, k, groups)
        return remote(
            near_out.at[k, j] if near else outgoing.at[other],
            arrived.at[ahead(j), k],
            asend.at[k, j],
            arecv.at[k, j],
            "sp",
            other,
        )

    def send_mix(j):
        return remote(mix, mix_far.at[j - 1], msend.at[j], mrecv.at[j], "tp", ahead(size - j))

    def place(k, who, whole):
        return rows_all.at[who] if whole else arrived.at[who, k]

    def near_copy(k, whole=False):
        src = stream if whole else arrived.at[me, k]
        return remote(src, place(k, me, whole), nsend.at[k], nrecv.at[k], "tp", partner)

    def far_copy(k, j, whole=False):
        src = stream if whole else arrived.at[me, k]
        return remote(
            src, place(k, me, whole), fsend.at[k, j], frecv.at[k, j], "tp", lax.rem(me + 2 * j, size)
        )

    def forward(k, j, whole=False):
        ref = place(k, lax.rem(me - 2 * j + size, size), whole)
        return remote(ref, ref, gsend.at[k, j], grecv.at[k, j], "tp", partner)

    def send_own(k, whole=False):
        for j in range(1, half):
            far_copy(k, j, whole).start()
        near_copy(k, whole).start()

    def pass_on(k, whole=False):
        for j in range(1, half):
            far_copy(k, j, whole).wait_recv()
            forward(k, j, whole).start()

    def gathered(k, whole=False):
        near_copy(k, whole).wait_recv()
        for j in range(1, half):
            forward(k, j, whole).wait_recv()

    def reduce_near(k, j, whole=False):
        src, dst = (extra, enear) if whole else (parts, near)
        index = 0 if whole else k
        return remote(
            src.at[lax.rem(partner + 2 * j, size), index],
            dst.at[j, index],
            rnsend.at[k, j],
            rnrecv.at[k, j],
            "tp",
            partner,
        )

    def reduce_far(k, j, whole=False):
        src, dst = (epair, efar) if whole else (pair, far)
        index = 0 if whole else k
        return remote(
            src.at[j - 1, index],
            dst.at[j - 1, index],
            rfsend.at[k, j],
            rfrecv.at[k, j],
            "tp",
            lax.rem(me + 2 * j, size),
        )

    def back(k, j=0, whose=None):
        other = flip(own, k, groups)
        where = own if whose is None else whose
        return remote(
            stage.at[k] if j == 0 else stage_far.at[j - 1, k],
            returned.at[where] if j == 0 else returned_far.at[j - 1, where],
            bsend.at[k, j],
            brecv.at[k, j],
            "sp",
            other,
        )

    def finish_close(k):
        for j in range(half):
            reduce_near(k, j).wait_recv()
            total = narrow(
                parts[ahead(j), k].astype(jnp.float32) + near[j, k].astype(jnp.float32)
            )

            @pl.when(k == 0)
            def _():
                if j == 0:
                    returned[own] = total
                else:
                    returned_far[j - 1, own] = total

            @pl.when(k > 0)
            def _():
                if j == 0:
                    stage[k] = total
                else:
                    stage_far[j - 1, k] = total
                back(k, j).start()

    def weighed(weights, rows):
        top, rest = split(weights)
        rows = narrow(rows.astype(jnp.float32).reshape(groups * block, width))
        return mm(top, rows) + mm(rest, rows)

    def add_extra():
        for k in range(1, close):
            for j in range(half):
                back(k, j, flip(own, k, groups)).wait_recv()
        for j in range(1, half):
            reduce_near(groups, j, True).wait_recv()
            send_mix(j).wait_recv()
            epair[j - 1, 0] = narrow(
                extra[ahead(j), 0].astype(jnp.float32)
                + enear[j, 0].astype(jnp.float32)
                + weighed(mix_far[j - 1], returned_far[j - 1])
            )
            reduce_far(groups, j, True).start()

    def start_reduce(k, whole=False):
        for j in range(half - 1, -1, -1):
            reduce_near(k, j, whole).start()

    def add_pair(k, whole=False):
        src, got, to = (extra, enear, epair) if whole else (parts, near, pair)
        index = 0 if whole else k
        for j in range(1, half):
            reduce_near(k, j, whole).wait_recv()
            to[j - 1, index] = narrow(
                src[lax.rem(me + 2 * j, size), index].astype(jnp.float32)
                + got[j, index].astype(jnp.float32)
            )
            reduce_far(k, j, whole).start()

    def total_of(k, whole=False):
        src, got, last = (extra, enear, efar) if whole else (parts, near, far)
        index = 0 if whole else k
        reduce_near(k, 0, whole).wait_recv()
        total = src[me, index].astype(jnp.float32) + got[0, index].astype(jnp.float32)
        for j in range(1, half):
            reduce_far(k, j, whole).wait_recv()
            total = total + last[j - 1, index].astype(jnp.float32)
        return total

    def swish(gated, lifted):
        return gated / (1.0 + jnp.exp(-gated)) * lifted

    lead, relay = min(4, steps), min(2, steps)
    send_own(groups, True)
    for k in range(close, groups):
        exchange(k).start()
    for j in range(1, half):
        send_mix(j).start()
    keep_rows.wait()
    pass_on(groups, True)
    for k in range(1, close):
        other = flip(own, k, groups)
        for j in range(half):
            picked = narrow(choice[ahead(j), pl.ds(pl.multiple_of(other * block, 8), block)])
            near_out[k, j] = narrow(mm(picked, rows_all[ahead(j)]))
            exchange(k, j, True).start()
    for k in range(close, lead * batch):
        exchange(k).wait_recv()
        send_own(k)
    gathered(groups, True)
    for who in range(size):
        picked = narrow(choice[who, pl.ds(pl.multiple_of(own * block, 8), block)])
        arrived[who, 0] = narrow(mm(picked, rows_all[who]))
    for fetch in fetches[:3]:
        fetch.wait()
    everyone = rows_all[...].reshape(size * tokens, width)
    hidden = narrow(swish(mm(everyone, cgate_v[...]), mm(everyone, cup_v[...])))
    extra[...] = narrow(mm(hidden, cdown_v[...])).reshape(size, 1, tokens, width)
    start_reduce(groups, True)
    for k in range(1, close):
        for j in range(half):
            exchange(k, j, True).wait_recv()
        near_copy(k).start()
        for j in range(1, half):
            forward(k, j).start()
    for k in range(close, relay * batch):
        pass_on(k)
    for fetch in fetches[3:]:
        fetch.wait()

    piece_rows = size * batch * block
    row = lax.broadcasted_iota(jnp.int32, (piece_rows, gate_v.shape[2]), 0)
    hosted = lax.div(lax.rem(row, block), capacity)

    def turn(t, carry):
        def each(base, action):
            for b in range(batch):
                action(base * batch + b)

        @pl.when(t + lead < steps)
        def _():
            def action(k):
                exchange(k).wait_recv()
                send_own(k)

            each(t + lead, action)

        @pl.when(t + relay < steps)
        def _():
            each(t + relay, pass_on)

        @pl.when(t < steps)
        def _():
            def arrive(k):
                @pl.when(k > 0)
                def _():
                    gathered(k)

            each(t, arrive)
            rows_in = narrow(
                arrived[:, pl.ds(t * batch, batch)].astype(jnp.float32).reshape(piece_rows, width)
            )
            hidden = []
            for expert in range(EXP_DEV):
                gated = mm(rows_in, gate_v[expert])
                lifted = mm(rows_in, up_v[expert])
                hidden.append(narrow(jnp.where(hosted == expert, swish(gated, lifted), 0.0)))
            part = mm(jnp.concatenate(hidden, 1), down_v[...].reshape(-1, width))
            parts[:, pl.ds(t * batch, batch)] = narrow(
                part.reshape(size, batch, block, width)
            )
            each(t, start_reduce)

        @pl.when((t >= 1) & (t <= steps))
        def _():
            def action(k):
                @pl.when(k < close)
                def _():
                    finish_close(k)

                @pl.when(k >= close)
                def _():
                    add_pair(k)

            each(t - 1, action)

        @pl.when(t == min(EXTRA_TURN, steps + 1))
        def _():
            add_extra()

        @pl.when(t >= 2)
        def _():
            def action(k):
                @pl.when(k >= close)
                def _():
                    stage[k] = narrow(total_of(k))
                    back(k).start()

            each(t - 2, action)

        return carry

    lax.fori_loop(0, steps + 2, turn, 0)

    shared = total_of(groups, True)
    for k in range(close, groups):
        back(k, 0, flip(own, k, groups)).wait_recv()
    out[...] = narrow(
        residual_scale * stream[...].astype(jnp.float32)
        + weighed(mix[...], returned[...])
        + shared
    )

    for k in range(1, groups):
        for j in range(half if k < close else 1):
            exchange(k, j, k < close).wait_send()
            back(k, j).wait_send()
    for k in range(groups + 1):
        whole = k == groups
        for j in range(half):
            reduce_near(k, j, whole).wait_send()
        if k > 0:
            near_copy(k, whole).wait_send()
        for j in range(1, half):
            if k > 0:
                forward(k, j, whole).wait_send()
            if k >= close:
                far_copy(k, j, whole).wait_send()
                reduce_far(k, j, whole).wait_send()
    for j in range(1, half):
        send_mix(j).wait_send()


def moe(
    choice, stream, mix, gate, upward, down, common_gate, common_up, common_down, capacity, block
):
    size = lax.axis_size("tp")
    groups = lax.axis_size("sp")
    tokens, width = stream.shape
    close = min(CLOSE, groups)
    half = size // 2
    dma = pltpu.SemaphoreType.DMA
    b16, f32 = jnp.bfloat16, jnp.float32
    anywhere = pl.BlockSpec(memory_space=pl.ANY)
    weights = (gate, upward, down, common_gate, common_up, common_down)
    return pl.pallas_call(
        lambda *refs: moe_kernel(size, groups, capacity, block, *refs),
        out_shape=jax.ShapeDtypeStruct((tokens, width), b16),
        in_specs=[VMEM] * 3 + [anywhere] * 6,
        out_specs=VMEM,
        scratch_shapes=[
            pltpu.VMEM((groups, block, width), b16),
            pltpu.VMEM((close, half, block, width), b16),
            pltpu.VMEM((half - 1,) + mix.shape, f32),
            pltpu.VMEM((half - 1, groups, block, width), b16),
            pltpu.VMEM((half - 1, close, block, width), b16),
            pltpu.VMEM((size, groups, block, width), b16),
            pltpu.VMEM((size, tokens, width), b16),
            pltpu.VMEM((size, groups, block, width), b16),
            pltpu.VMEM((half, groups, block, width), b16),
            pltpu.VMEM((half - 1, groups, block, width), b16),
            pltpu.VMEM((half - 1, groups, block, width), b16),
            pltpu.VMEM((groups, block, width), b16),
            pltpu.VMEM((groups, block, width), b16),
            pltpu.VMEM((size, 1, tokens, width), b16),
            pltpu.VMEM((half, 1, tokens, width), b16),
            pltpu.VMEM((half - 1, 1, tokens, width), b16),
            pltpu.VMEM((half - 1, 1, tokens, width), b16),
        ]
        + [pltpu.VMEM(w.shape, b16) for w in weights]
        + [dma((2,)), dma((6,)), dma((groups, half)), dma((groups, half))]
        + [dma((groups + 1,))] * 2
        + [dma((groups + 1, half))] * 8
        + [dma((groups, half))] * 2
        + [dma((half,))] * 2,
        compiler_params=pltpu.CompilerParams(
            collective_id=4, has_side_effects=True, vmem_limit_bytes=60 * 1024 * 1024
        ),
    )(choice, stream, mix, *weights)


def per_device(
    head_queries,
    head_keys,
    head_values,
    decay_logits,
    learning_logits,
    surge_decay,
    documents,
    residual,
    head_norm_scale,
    mixer_output_weight,
    layer_norm_scale,
    routes,
    routing_weight,
    routed_gate_weight,
    routed_up_weight,
    routed_down_weight,
    common_gate_weight,
    common_up_weight,
    common_down_weight,
):
    head_outputs = mixer(
        head_queries,
        head_keys,
        head_values,
        decay_logits,
        learning_logits,
        surge_decay,
        documents,
        head_norm_scale,
    )
    quarters = lax.axis_size("tp")
    groups = lax.axis_size("sp")
    own_rows, model_width = residual.shape
    pieces = own_rows // 16
    mixed_parts = jnp.dot(
        head_outputs, mixer_output_weight, preferred_element_type=jnp.float32
    ).astype(jnp.bfloat16)
    mixed_rows = tp_reduce(mixed_parts.reshape(quarters, pieces, 16, model_width)).reshape(
        own_rows, model_width
    )
    summed = residual_scale * residual.astype(jnp.float32) + mixed_rows
    centre = jnp.mean(summed, -1, keepdims=True)
    spread = jnp.mean(jnp.square(summed - centre), -1, keepdims=True)
    stream = ((summed - centre) * lax.rsqrt(spread + norm_eps) * layer_norm_scale).astype(
        jnp.bfloat16
    )
    experts = EXP_DEV * groups
    capacity = max(2, (3 * TOK_DEV * TOP + 2 * experts - 1) // (2 * experts))
    block_rows = 8 * ((EXP_DEV * capacity + 7) // 8)
    chosen = routes.reshape(quarters, own_rows * TOP)
    onehot = (chosen[..., None] == jnp.arange(experts, dtype=jnp.int32)).astype(jnp.int32)
    ranking = jnp.sum(jnp.cumsum(onehot, 1) * onehot, -1) - 1
    slot_index = (
        chosen // EXP_DEV * block_rows + chosen % EXP_DEV * capacity + ranking
    )
    slot_index = slot_index.reshape(quarters, own_rows, TOP)
    own_slots = lax.dynamic_index_in_dim(slot_index, lax.axis_index("tp"), 0, keepdims=False)
    slots = jnp.arange(groups * block_rows, dtype=jnp.int32)
    hits = own_slots[:, :, None] == slots
    choice = jnp.zeros((quarters, groups * block_rows, own_rows), jnp.float32)
    for route in range(TOP):
        choice = choice + (slots[None, :, None] == slot_index[:, None, :, route])
    weights = jnp.sum(jnp.where(hits, routing_weight[:, :, None], 0.0), 1)
    return moe(
        choice,
        stream,
        weights,
        routed_gate_weight,
        routed_up_weight,
        routed_down_weight,
        common_gate_weight,
        common_up_weight,
        common_down_weight,
        capacity,
        block_rows,
    )


def solution(mesh):
    placed = (
        P("sp", "tp"),
        P("sp", "tp"),
        P("sp", "tp"),
        P("sp", "tp"),
        P("sp", "tp"),
        P("sp", "tp"),
        P("sp"),
        P(("sp", "tp"), None),
        P("tp"),
        P("tp", None),
        P(),
        P("sp", None),
        P(("sp", "tp"), None),
        P("sp", None, "tp"),
        P("sp", None, "tp"),
        P("sp", "tp", None),
        P(None, "tp"),
        P(None, "tp"),
        P("tp", None),
    )
    return jax.shard_map(
        per_device, mesh=mesh, in_specs=placed, out_specs=P(("sp", "tp"), None), check_vma=False
    )
```

```python
import jax
import jax.numpy as jnp
from jax import lax
from jax.experimental import pallas as pl
from jax.experimental.pallas import tpu as pltpu
from jax.sharding import PartitionSpec as P

HEAD = 64
EXP_DEV = 2
TOP = 2
BLOCK_SPAN = 64
TOK_DEV = 64


residual_scale = 2.0**0.5
group_eps = 0.00064
norm_eps = 1e-05
unit_eps = 1e-06
CLOSE = 2
EXTRA_TURN = 5
SCORE_PRECISION = lax.Precision.HIGH


MESH = pl.DeviceIdType.MESH
VMEM = pl.BlockSpec(memory_space=pltpu.VMEM)


def remote(src, dst, send_sem, recv_sem, axis, index):
    return pltpu.make_async_remote_copy(
        src_ref=src,
        dst_ref=dst,
        send_sem=send_sem,
        recv_sem=recv_sem,
        device_id={axis: index},
        device_id_type=MESH,
    )


def chunk_iota(rows, cols, dim):
    return lax.broadcasted_iota(jnp.int32, (rows, cols), dim)


def mm(left, right, precision=None):
    return jnp.dot(left, right, preferred_element_type=jnp.float32, precision=precision)


def mm_nt(left, right, precision=None):
    return lax.dot_general(
        left,
        right,
        (((1,), (1,)), ((), ())),
        preferred_element_type=jnp.float32,
        precision=precision,
    )


def mm_tn(left, right, precision=None):
    return lax.dot_general(
        left,
        right,
        (((0,), (0,)), ((), ())),
        preferred_element_type=jnp.float32,
        precision=precision,
    )


def narrow(values):
    return values.astype(jnp.bfloat16)


def split(values):
    top = narrow(values)
    return top, narrow(values - top.astype(jnp.float32))


def mixer_body(
    size,
    sides,
    block,
    capacity,
    queries,
    keys,
    values,
    decays,
    rates,
    surges,
    docs,
    scale,
    out_weight,
    residual,
    layer_scale,
    routes,
    route_weight,
    meet,
    stream,
    choice,
    mix,
    ahead_s,
    fwd_s,
    reads_s,
    solved_s,
    map_s,
    add_s,
    local_s,
    starts_s,
    comp_s,
    far_s,
    join_s,
    doc_out,
    doc_in,
    padd_out,
    padd_in,
    pmap_out,
    pmap_in,
    s_out,
    s_in,
    mixed,
    mixed_near,
    mixed_pair,
    mixed_far,
    doc_sem,
    padd_sem,
    pmap_sem,
    near_sem,
    next_sem,
    s_recv,
    mn_sem,
    mf_sem,
):
    me = lax.axis_index("sp")
    span = BLOCK_SPAN
    rows, width = queries.shape
    chunks = rows // span
    lanes = 2 * HEAD
    pairs = width // lanes
    heads = rates.shape[0]
    high = lax.Precision.HIGH
    same_half = (chunk_iota(lanes, lanes, 0) // HEAD) == (chunk_iota(lanes, lanes, 1) // HEAD)
    ones_half = same_half.astype(jnp.float32)
    earlier = lax.rem(chunk_iota(span, lanes, 1), HEAD)
    later = chunk_iota(span, lanes, 0)
    unit_pair = (earlier == later).astype(jnp.float32)
    unit_full = (chunk_iota(lanes, lanes, 0) == chunk_iota(lanes, lanes, 1)).astype(jnp.float32)

    def wide(block):
        return jnp.where(same_half, jnp.concatenate([block, block], 0), 0.0)

    row_docs = docs[...].astype(jnp.float32)
    row_square = jnp.broadcast_to(row_docs, (rows, rows))
    diag = chunk_iota(rows, rows, 0) == chunk_iota(rows, rows, 1)
    doc_col = mm(
        narrow(jnp.where(diag, row_square, 0.0)), jnp.ones((rows, lanes), jnp.bfloat16)
    )
    pick = (
        lax.rem(chunk_iota(rows, lanes, 0), span) == lax.rem(chunk_iota(rows, lanes, 1), HEAD)
    ).astype(jnp.bfloat16)
    wide_rows = 8 * ((chunks + 7) // 8)
    in_chunk = (chunk_iota(wide_rows, rows, 1) // span) == chunk_iota(wide_rows, rows, 0)
    doc_row = mm(
        narrow(jnp.where(in_chunk, jnp.broadcast_to(row_docs, (wide_rows, rows)), 0.0)), pick
    )
    same_chunk = (chunk_iota(rows, rows, 0) // span) == (chunk_iota(rows, rows, 1) // span)
    tri = (
        (chunk_iota(rows, rows, 0) >= chunk_iota(rows, rows, 1)) & same_chunk
    ).astype(jnp.bfloat16)

    strict, causal, joined, tail = [], [], [], []
    for c in range(chunks):
        col = doc_col[c * span : (c + 1) * span]
        same_doc = col == doc_row[c : c + 1]
        strict.append(same_doc & (later > earlier))
        causal.append(same_doc & (later >= earlier))
        before_row = doc_col[max(c * span - 1, 0) : max(c * span - 1, 0) + 1]
        joined.append((col == before_row).astype(jnp.float32))
        tail.append((col == doc_col[(c + 1) * span - 1 : (c + 1) * span]).astype(jnp.float32))

    doc_out[...] = jnp.broadcast_to(doc_col[rows - 1 : rows], doc_out.shape)
    meet()
    following = lax.rem(me + 1, size)
    doc_hop = remote(doc_out, doc_in, doc_sem.at[0], doc_sem.at[1], "sp", following)

    @pl.when(me < size - 1)
    def _():
        doc_hop.start()

    rate_all = jax.nn.sigmoid(rates[...].astype(jnp.float32))
    surge_all = surges[...]

    def local_pairs(turn, carry):
        streams = []
        for half in range(2):
            p = turn * 2 + half
            cols = pl.ds(pl.multiple_of(p * lanes, lanes), lanes)
            spread_heads = (
                chunk_iota(heads, lanes, 0) == 2 * p + chunk_iota(heads, lanes, 1) // HEAD
            ).astype(jnp.float32)
            key = keys[:, cols].astype(jnp.float32)
            norm = mm(key * key, ones_half, high)
            unit = key * lax.rsqrt(norm + unit_eps)
            rate = mm_tn(rate_all, spread_heads, high)
            surge = mm_tn(surge_all, spread_heads, high)
            logit = decays[:, cols].astype(jnp.float32)
            decay = surge - jnp.exp(-0.5) / (1.0 + jnp.exp(-logit))
            top, rest = split(decay)
            cumulative = mm(tri, top) + mm(tri, rest)
            grown = jnp.exp(cumulative)
            shrunk = jnp.exp(-cumulative)
            ahead = unit * jnp.exp(cumulative - decay)
            unit_rate = unit * rate
            back_unit = unit_rate * shrunk
            back_key = key * shrunk
            forward = queries[:, cols].astype(jnp.float32) * grown
            ahead_s[:, cols] = ahead
            fwd_s[:, cols] = forward
            for c in range(chunks):
                part = slice(c * span, (c + 1) * span)
                total = cumulative[(c + 1) * span - 1 : (c + 1) * span]
                ending = jnp.exp(total - cumulative[part]) * tail[c]
                streams.append(
                    dict(
                        c=c,
                        p=p,
                        cols=cols,
                        ahead=ahead[part],
                        fwd=forward[part],
                        bu=back_unit[part],
                        bk=back_key[part],
                        eu=-unit_rate[part] * ending,
                        ek=key[part] * ending,
                        val=values[part, cols].astype(jnp.float32),
                        keep=jnp.exp(total) * joined[c][span - 1 : span],
                    )
                )
        for s in streams:
            c = s["c"]
            scores = mm_nt(
                jnp.concatenate([s["ahead"], s["fwd"]], 0),
                jnp.concatenate([wide(s["bu"]), wide(s["bk"])], 0),
                SCORE_PRECISION,
            )
            s["low"] = jnp.where(strict[c], scores[:span, :lanes], 0.0)
            s["mixk"] = jnp.where(strict[c], scores[:span, lanes:], 0.0)
            reads_s[c, s["p"], :, :lanes] = narrow(
                jnp.where(causal[c], -scores[span:, :lanes], 0.0)
            )
            reads_s[c, s["p"], :, lanes:] = narrow(jnp.where(causal[c], scores[span:, lanes:], 0.0))
        base = 16
        near_block = (earlier // base) == (later // base)
        for s in streams:
            s["low_near"] = jnp.where(near_block, s["low"], 0.0)
            s["inv"] = unit_pair - s["low_near"]
        for s in streams:
            s["power"] = mm(s["low_near"], wide(s["low_near"]), high)
            s["mv"] = mm(s["mixk"], wide(s["val"]))
        reach = 2
        while reach < base:
            last = reach * 2 >= base
            for s in streams:
                right = wide(s["power"])
                if last:
                    s["inv"] = s["inv"] + mm(s["inv"], right, high)
                else:
                    both = mm(jnp.concatenate([s["power"], s["inv"]], 0), right, high)
                    s["power"] = both[:span]
                    s["inv"] = s["inv"] + both[span:]
            reach = reach * 2
        while base < span:
            off = ((earlier // base) != (later // base)) & (
                (earlier // (2 * base)) == (later // (2 * base))
            )
            for s in streams:
                s["mid"] = mm(s["inv"], wide(jnp.where(off, s["low"], 0.0)), high)
            for s in streams:
                s["inv"] = s["inv"] - mm(s["mid"], wide(s["inv"]), high)
            base = base * 2
        for s in streams:
            c = s["c"]
            s["solved"] = mm(
                s["inv"],
                jnp.concatenate([wide(s["ahead"] * joined[c]), wide(s["mv"])], 1),
                high,
            )
            solved_s[c, s["p"]] = narrow(s["solved"])
        for s in streams:
            c, p = s["c"], s["p"]
            pull = mm_tn(s["solved"][:, :lanes], s["eu"], high)
            map_s[c, p] = jnp.where(same_half, pull, 0.0) + unit_full * s["keep"]
            grown = mm_tn(
                jnp.concatenate([s["solved"][:, lanes:], s["val"]], 0),
                jnp.concatenate([s["eu"], s["ek"]], 0),
                high,
            )
            grown = jnp.where(same_half, grown, 0.0)
            add_s[c, p] = grown[:HEAD] + grown[HEAD:]
        return carry

    lax.fori_loop(0, pairs // 2, local_pairs, 0)

    state = [None] * pairs
    for p in range(pairs):
        state[p] = jnp.concatenate([add_s[0, p], map_s[0, p][:HEAD] + map_s[0, p][HEAD:]], 0)
    kept = [state]
    for c in range(1, chunks):
        state = [
            mm(kept[-1][p], map_s[c, p], high)
            + jnp.concatenate([add_s[c, p], jnp.zeros((HEAD, lanes), jnp.float32)], 0)
            for p in range(pairs)
        ]
        kept.append(state)
    finals = kept[-1]

    @pl.when(me == 0)
    def _():
        join_s[...] = jnp.zeros_like(join_s)
        s_in[...] = jnp.zeros_like(s_in)

    @pl.when(me > 0)
    def _():
        doc_hop.wait_recv()
        join_s[...] = (doc_in[...] == doc_col[0:1]).astype(jnp.float32)

    join = join_s[0:1]
    for p in range(pairs):
        comp_s[p] = jnp.concatenate([finals[p][:HEAD], finals[p][HEAD:] * join], 0)
    even = lax.rem(me, 2) == 0

    def pair_hop(p):
        return (
            remote(padd_out.at[p], padd_in.at[p], padd_sem.at[0, p], padd_sem.at[1, p], "sp", following),
            remote(pmap_out.at[p], pmap_in.at[p], pmap_sem.at[0, p], pmap_sem.at[1, p], "sp", following),
        )

    def state_hop(p, near):
        sem = near_sem if near else next_sem
        return remote(
            s_out.at[p],
            s_in.at[p],
            sem.at[p],
            s_recv.at[p],
            "sp",
            lax.rem(me + (2 if near else 1), size),
        )

    @pl.when(even)
    def _():
        for p in range(pairs):
            padd_out[p] = narrow(comp_s[p, :HEAD])
            pmap_out[p] = comp_s[p, HEAD:]
        for p in range(pairs):
            pair_hop(p)[0].start()
        for p in range(pairs):
            pair_hop(p)[1].start()

    def finish_local():
        for p in range(pairs):
            cols = slice(p * lanes, (p + 1) * lanes)
            for c in range(chunks):
                part = slice(c * span, (c + 1) * span)
                read_unit = reads_s[c, p, :, :lanes]
                solved = solved_s[c, p].astype(jnp.float32)
                local = mm(
                    reads_s[c, p],
                    jnp.concatenate(
                        [
                            narrow(wide(solved[:, lanes:])),
                            narrow(wide(values[part, cols].astype(jnp.float32))),
                        ],
                        0,
                    ),
                )
                start = fwd_s[part, cols] * joined[c] + mm(
                    read_unit, narrow(wide(solved[:, :lanes]))
                )
                if c > 0:
                    seen = mm_nt(
                        narrow(start),
                        jnp.concatenate(
                            [
                                narrow(wide(kept[c - 1][p][:HEAD])),
                                narrow(wide(kept[c - 1][p][HEAD:])),
                            ],
                            0,
                        ),
                    )
                    local = local + seen[:, :lanes]
                    start = seen[:, lanes:]
                local_s[part, cols] = local
                starts_s[part, cols] = narrow(start)

    finish_local()

    own_tp = lax.axis_index("tp")
    tokens = residual.shape[0]
    experts = EXP_DEV * size
    slot_list = size * block
    named = routes[...].astype(jnp.float32)
    expert_row = chunk_iota(experts, rows, 0).astype(jnp.float32)
    taken = jnp.zeros((experts, rows), jnp.float32)
    for route in range(TOP):
        taken = taken + (named[route : route + 1] == expert_row).astype(jnp.float32)
    same_block = (chunk_iota(rows, rows, 0) // tokens) == (chunk_iota(rows, rows, 1) // tokens)
    prior = ((chunk_iota(rows, rows, 0) < chunk_iota(rows, rows, 1)) & same_block).astype(
        jnp.bfloat16
    )
    taken = narrow(taken)
    rank = narrow(mm(taken, prior))
    place = lax.rem(chunk_iota(slot_list, experts, 0), block)
    hosts = ((chunk_iota(slot_list, experts, 0) // block) * EXP_DEV + place // capacity) == (
        chunk_iota(slot_list, experts, 1)
    )
    hosts = (hosts & (place < EXP_DEV * capacity)).astype(jnp.float32)
    seat = lax.rem(lax.rem(chunk_iota(slot_list, rows, 0), block), capacity).astype(jnp.float32)
    chosen = narrow(
        jnp.where(
            (mm(narrow(hosts), taken) > 0.5) & (mm(narrow(hosts), rank) == seat), 1.0, 0.0
        )
    )

    def part_of(who):
        return (
            chunk_iota(rows, tokens, 0) == who * tokens + chunk_iota(rows, tokens, 1)
        ).astype(jnp.bfloat16)

    for who in range(sides):
        choice[who] = mm(chosen, part_of(who))
    named_own = mm(narrow(named), part_of(own_tp))
    expert_own = chunk_iota(experts, tokens, 0).astype(jnp.float32)
    amount = jnp.zeros((experts, tokens), jnp.float32)
    for route in range(TOP):
        amount = amount + jnp.where(
            named_own[route : route + 1] == expert_own, route_weight[route : route + 1, :], 0.0
        )
    mix[...] = choice[own_tp] * mm(hosts, amount, lax.Precision.HIGHEST)

    @pl.when(jnp.logical_not(even))
    def _():
        for p in range(pairs):
            pair_hop(p)[0].wait_recv()
            first = padd_in[p]
            top, rest = split(wide(comp_s[p, HEAD:]))
            far_s[p, :HEAD] = (
                mm(jnp.concatenate([first, first], 1), jnp.concatenate([top, rest], 0))
                + comp_s[p, :HEAD]
            )

        @pl.when(me == 1)
        def _():
            s_in[...] = jnp.zeros_like(s_in)
            for p in range(pairs):
                s_out[p] = narrow(far_s[p, :HEAD])
                state_hop(p, True).start()

        for p in range(pairs):
            pair_hop(p)[1].wait_recv()

        @pl.when(me > 1)
        def _():
            for p in range(pairs):
                both = mm(pmap_in[p], wide(comp_s[p, HEAD:]), high)
                far_s[p, HEAD:] = both
            weights = []
            for p in range(pairs):
                top, rest = split(wide(far_s[p, HEAD:]))
                weights.append(jnp.concatenate([top, rest], 0))
            for p in range(pairs):
                state_hop(p, True).wait_recv()

                @pl.when(me < size - 1)
                def _():
                    arrived = s_in[p]
                    s_out[p] = narrow(
                        mm(jnp.concatenate([arrived, arrived], 1), weights[p]) + far_s[p, :HEAD]
                    )
                    state_hop(p, True).start()

        @pl.when(me < size - 1)
        def _():
            for p in range(pairs):
                state_hop(p, False).start()

        for p in range(pairs):
            top, rest = split(wide(pmap_in[p]))
            arrived = s_in[p]
            comp_s[p, :HEAD] = (
                mm(jnp.concatenate([arrived, arrived], 1), jnp.concatenate([top, rest], 0))
                + padd_in[p].astype(jnp.float32)
            )

    @pl.when(even)
    def _():
        @pl.when(me > 0)
        def _():
            for p in range(pairs):
                state_hop(p, False).wait_recv()

        for p in range(pairs):
            comp_s[p, :HEAD] = s_in[p].astype(jnp.float32)

    half = sides // 2
    partner = own_tp + 1 - 2 * lax.rem(own_tp, 2)
    split_rows = 16
    split_list = tokens // split_rows

    def ahead(j, who=None):
        return lax.rem((own_tp if who is None else who) + 2 * j, sides)

    def near_hop(j):
        return remote(
            mixed.at[ahead(j, partner)], mixed_near.at[j], mn_sem.at[0, j], mn_sem.at[1, j], "tp", partner
        )

    def far_hop(j, i):
        span_rows = pl.ds(i * split_rows, split_rows)
        return remote(
            mixed_pair.at[j - 1, span_rows],
            mixed_far.at[j - 1, span_rows],
            mf_sem.at[0, j, i],
            mf_sem.at[1, j, i],
            "tp",
            ahead(j),
        )

    incoming = [narrow(wide(comp_s[p, :HEAD] * join)) for p in range(pairs)]

    def project(quarter):
        part = pl.ds(pl.multiple_of(quarter * tokens, tokens), tokens)
        normed = []
        for p in range(pairs):
            cols = slice(p * lanes, (p + 1) * lanes)
            read = local_s[part, cols] + mm_nt(starts_s[part, cols], incoming[p])
            centred = read - mm(read, ones_half, high) * (1.0 / HEAD)
            spread = mm(centred * centred, ones_half, high) * (1.0 / HEAD)
            normed.append(
                narrow(centred * lax.rsqrt(spread + group_eps) * scale[:, cols])
            )
        mixed[quarter] = narrow(mm(jnp.concatenate(normed, 1), out_weight[...]))

    for j in range(half - 1, -1, -1):
        project(ahead(j, partner))
        near_hop(j).start()
        project(ahead(j))
        if j > 0:
            near_hop(j).wait_recv()
            for i in range(split_list):
                take = slice(i * split_rows, (i + 1) * split_rows)
                mixed_pair[j - 1, take] = narrow(
                    mixed[ahead(j), take].astype(jnp.float32)
                    + mixed_near[j, take].astype(jnp.float32)
                )
                far_hop(j, i).start()
    near_hop(0).wait_recv()
    for i in range(split_list):
        take = slice(i * split_rows, (i + 1) * split_rows)
        total = (
            residual_scale * residual[take].astype(jnp.float32)
            + mixed[own_tp, take].astype(jnp.float32)
            + mixed_near[0, take].astype(jnp.float32)
        )
        for j in range(1, half):
            far_hop(j, i).wait_recv()
            total = total + mixed_far[j - 1, take].astype(jnp.float32)
        centred = total - jnp.mean(total, -1, keepdims=True)
        spread = jnp.mean(centred * centred, -1, keepdims=True)
        stream[take] = narrow(centred * lax.rsqrt(spread + norm_eps) * layer_scale[...])

    for j in range(half):
        near_hop(j).wait_send()
        if j > 0:
            for i in range(split_list):
                far_hop(j, i).wait_send()

    @pl.when(me < size - 1)
    def _():
        doc_hop.wait_send()

    @pl.when(even)
    def _():
        for p in range(pairs):
            for hop in pair_hop(p):
                hop.wait_send()

    @pl.when(jnp.logical_not(even) & (me < size - 1))
    def _():
        for p in range(pairs):
            state_hop(p, True).wait_send()
            state_hop(p, False).wait_send()


def flip(index, bits, size):
    total = 0
    place = 1
    while place < size:
        total = total + lax.rem(lax.div(index, place) + lax.div(bits, place), 2) * place
        place = place * 2
    return total


def moe_body(
    size,
    groups,
    capacity,
    block,
    fetches,
    choice,
    stream,
    mix,
    out,
    outgoing,
    near_out,
    returned_far,
    mix_far,
    stage_far,
    arrived,
    rows_all,
    parts,
    near,
    pair,
    far,
    stage,
    returned,
    extra,
    enear,
    epair,
    efar,
    cgate_v,
    cup_v,
    cdown_v,
    gate_v,
    up_v,
    down_v,
    local,
    asend,
    arecv,
    nsend,
    nrecv,
    fsend,
    frecv,
    gsend,
    grecv,
    rnsend,
    rnrecv,
    rfsend,
    rfrecv,
    bsend,
    brecv,
    msend,
    mrecv,
):
    me = lax.axis_index("tp")
    own = lax.axis_index("sp")
    half = size // 2
    partner = me + 1 - 2 * lax.rem(me, 2)
    tokens, width = stream.shape
    close = min(CLOSE, groups)
    batch = max(1, groups // 8)
    steps = groups // batch
    keep_rows = pltpu.make_async_copy(stream, rows_all.at[me], local.at[1])
    keep_rows.start()
    outgoing[...] = narrow(mm(narrow(choice[me]), stream[...])).reshape(groups, block, width)
    def ahead(j):
        return lax.rem(me + 2 * j, size)

    def exchange(k, j=0, near=False):
        other = flip(own, k, groups)
        return remote(
            near_out.at[k, j] if near else outgoing.at[other],
            arrived.at[ahead(j), k],
            asend.at[k, j],
            arecv.at[k, j],
            "sp",
            other,
        )

    def send_mix(j):
        return remote(mix, mix_far.at[j - 1], msend.at[j], mrecv.at[j], "tp", ahead(size - j))

    def place(k, who, whole):
        return rows_all.at[who] if whole else arrived.at[who, k]

    def near_copy(k, whole=False):
        src = stream if whole else arrived.at[me, k]
        return remote(src, place(k, me, whole), nsend.at[k], nrecv.at[k], "tp", partner)

    def far_copy(k, j, whole=False):
        src = stream if whole else arrived.at[me, k]
        return remote(
            src, place(k, me, whole), fsend.at[k, j], frecv.at[k, j], "tp", lax.rem(me + 2 * j, size)
        )

    def forward(k, j, whole=False):
        ref = place(k, lax.rem(me - 2 * j + size, size), whole)
        return remote(ref, ref, gsend.at[k, j], grecv.at[k, j], "tp", partner)

    def send_own(k, whole=False):
        for j in range(1, half):
            far_copy(k, j, whole).start()
        near_copy(k, whole).start()

    def pass_on(k, whole=False):
        for j in range(1, half):
            far_copy(k, j, whole).wait_recv()
            forward(k, j, whole).start()

    def gathered(k, whole=False):
        near_copy(k, whole).wait_recv()
        for j in range(1, half):
            forward(k, j, whole).wait_recv()

    def reduce_near(k, j, whole=False):
        src, dst = (extra, enear) if whole else (parts, near)
        index = 0 if whole else k
        return remote(
            src.at[lax.rem(partner + 2 * j, size), index],
            dst.at[j, index],
            rnsend.at[k, j],
            rnrecv.at[k, j],
            "tp",
            partner,
        )

    def reduce_far(k, j, whole=False):
        src, dst = (epair, efar) if whole else (pair, far)
        index = 0 if whole else k
        return remote(
            src.at[j - 1, index],
            dst.at[j - 1, index],
            rfsend.at[k, j],
            rfrecv.at[k, j],
            "tp",
            lax.rem(me + 2 * j, size),
        )

    def back(k, j=0, whose=None):
        other = flip(own, k, groups)
        where = own if whose is None else whose
        return remote(
            stage.at[k] if j == 0 else stage_far.at[j - 1, k],
            returned.at[where] if j == 0 else returned_far.at[j - 1, where],
            bsend.at[k, j],
            brecv.at[k, j],
            "sp",
            other,
        )

    def finish_close(k):
        for j in range(half):
            reduce_near(k, j).wait_recv()
            total = narrow(
                parts[ahead(j), k].astype(jnp.float32) + near[j, k].astype(jnp.float32)
            )

            @pl.when(k == 0)
            def _():
                if j == 0:
                    returned[own] = total
                else:
                    returned_far[j - 1, own] = total

            @pl.when(k > 0)
            def _():
                if j == 0:
                    stage[k] = total
                else:
                    stage_far[j - 1, k] = total
                back(k, j).start()

    def weighed(weights, rows):
        top, rest = split(weights)
        rows = narrow(rows.astype(jnp.float32).reshape(groups * block, width))
        return mm_tn(top, rows) + mm_tn(rest, rows)

    def add_extra():
        for k in range(1, close):
            for j in range(half):
                back(k, j, flip(own, k, groups)).wait_recv()
        for j in range(1, half):
            reduce_near(groups, j, True).wait_recv()
            send_mix(j).wait_recv()
            epair[j - 1, 0] = narrow(
                extra[ahead(j), 0].astype(jnp.float32)
                + enear[j, 0].astype(jnp.float32)
                + weighed(mix_far[j - 1], returned_far[j - 1])
            )
            reduce_far(groups, j, True).start()

    def start_reduce(k, whole=False):
        for j in range(half - 1, -1, -1):
            reduce_near(k, j, whole).start()

    def add_pair(k, whole=False):
        src, got, to = (extra, enear, epair) if whole else (parts, near, pair)
        index = 0 if whole else k
        for j in range(1, half):
            reduce_near(k, j, whole).wait_recv()
            to[j - 1, index] = narrow(
                src[lax.rem(me + 2 * j, size), index].astype(jnp.float32)
                + got[j, index].astype(jnp.float32)
            )
            reduce_far(k, j, whole).start()

    def total_of(k, whole=False):
        src, got, last = (extra, enear, efar) if whole else (parts, near, far)
        index = 0 if whole else k
        reduce_near(k, 0, whole).wait_recv()
        total = src[me, index].astype(jnp.float32) + got[0, index].astype(jnp.float32)
        for j in range(1, half):
            reduce_far(k, j, whole).wait_recv()
            total = total + last[j - 1, index].astype(jnp.float32)
        return total

    def swish(gated, lifted):
        return gated / (1.0 + jnp.exp(-gated)) * lifted

    lead, relay = min(4, steps), min(2, steps)
    send_own(groups, True)
    for k in range(close, groups):
        exchange(k).start()
    for j in range(1, half):
        send_mix(j).start()
    keep_rows.wait()
    pass_on(groups, True)
    for k in range(1, close):
        other = flip(own, k, groups)
        for j in range(half):
            picked = narrow(choice[ahead(j), pl.ds(pl.multiple_of(other * block, 8), block)])
            near_out[k, j] = narrow(mm(picked, rows_all[ahead(j)]))
            exchange(k, j, True).start()
    for k in range(close, lead * batch):
        exchange(k).wait_recv()
        send_own(k)
    gathered(groups, True)
    for who in range(size):
        picked = narrow(choice[who, pl.ds(pl.multiple_of(own * block, 8), block)])
        arrived[who, 0] = narrow(mm(picked, rows_all[who]))
    for fetch in fetches[:3]:
        fetch.wait()
    everyone = rows_all[...].reshape(size * tokens, width)
    hidden = narrow(swish(mm(everyone, cgate_v[...]), mm(everyone, cup_v[...])))
    extra[...] = narrow(mm(hidden, cdown_v[...])).reshape(size, 1, tokens, width)
    start_reduce(groups, True)
    for k in range(1, close):
        for j in range(half):
            exchange(k, j, True).wait_recv()
        near_copy(k).start()
        for j in range(1, half):
            forward(k, j).start()
    for k in range(close, relay * batch):
        pass_on(k)
    for fetch in fetches[3:]:
        fetch.wait()

    piece_rows = size * batch * block
    row = lax.broadcasted_iota(jnp.int32, (piece_rows, gate_v.shape[2]), 0)
    hosted = lax.div(lax.rem(row, block), capacity)

    def turn(t, carry):
        def each(base, action):
            for b in range(batch):
                action(base * batch + b)

        @pl.when(t + lead < steps)
        def _():
            def action(k):
                exchange(k).wait_recv()
                send_own(k)

            each(t + lead, action)

        @pl.when(t + relay < steps)
        def _():
            each(t + relay, pass_on)

        @pl.when(t < steps)
        def _():
            def arrive(k):
                @pl.when(k > 0)
                def _():
                    gathered(k)

            each(t, arrive)
            rows_in = narrow(
                arrived[:, pl.ds(t * batch, batch)].astype(jnp.float32).reshape(piece_rows, width)
            )
            hidden = []
            for expert in range(EXP_DEV):
                gated = mm(rows_in, gate_v[expert])
                lifted = mm(rows_in, up_v[expert])
                hidden.append(narrow(jnp.where(hosted == expert, swish(gated, lifted), 0.0)))
            part = mm(jnp.concatenate(hidden, 1), down_v[...].reshape(-1, width))
            parts[:, pl.ds(t * batch, batch)] = narrow(
                part.reshape(size, batch, block, width)
            )
            each(t, start_reduce)

        @pl.when((t >= 1) & (t <= steps))
        def _():
            def action(k):
                @pl.when(k < close)
                def _():
                    finish_close(k)

                @pl.when(k >= close)
                def _():
                    add_pair(k)

            each(t - 1, action)

        @pl.when(t == min(EXTRA_TURN, steps + 1))
        def _():
            add_extra()

        @pl.when(t >= 2)
        def _():
            def action(k):
                @pl.when(k >= close)
                def _():
                    stage[k] = narrow(total_of(k))
                    back(k).start()

            each(t - 2, action)

        return carry

    lax.fori_loop(0, steps + 2, turn, 0)

    shared = total_of(groups, True)
    for k in range(close, groups):
        back(k, 0, flip(own, k, groups)).wait_recv()
    out[...] = narrow(
        residual_scale * stream[...].astype(jnp.float32)
        + weighed(mix[...], returned[...])
        + shared
    )

    for k in range(1, groups):
        for j in range(half if k < close else 1):
            exchange(k, j, k < close).wait_send()
            back(k, j).wait_send()
    for k in range(groups + 1):
        whole = k == groups
        for j in range(half):
            reduce_near(k, j, whole).wait_send()
        if k > 0:
            near_copy(k, whole).wait_send()
        for j in range(1, half):
            if k > 0:
                forward(k, j, whole).wait_send()
            if k >= close:
                far_copy(k, j, whole).wait_send()
                reduce_far(k, j, whole).wait_send()
    for j in range(1, half):
        send_mix(j).wait_send()


def layer_kernel(size, sides, block, capacity, counts, *refs):
    refs = list(refs)

    def take(count):
        got = refs[:count]
        del refs[:count]
        return got

    mixer_in = take(12)
    big = take(7)
    (out,) = take(1)
    big_v = take(7)
    (loads,) = take(1)
    meeting = take(3)
    mixer_scratch = take(counts[0])
    moe_scratch = take(counts[1])
    returned_far = moe_scratch[2]
    fetches = [
        pltpu.make_async_copy(src, dst, loads.at[i]) for i, (src, dst) in enumerate(zip(big, big_v))
    ]
    for fetch in fetches:
        fetch.start()
    returned_far[...] = jnp.zeros_like(returned_far)
    barrier = pltpu.get_barrier_semaphore()
    peers = 0
    for axis, number in (("sp", size), ("tp", sides)):
        here = lax.axis_index(axis)
        for step in range(1, number):
            pl.semaphore_signal(
                barrier,
                inc=1,
                device_id={axis: lax.rem(here + step, number)},
                device_id_type=MESH,
            )
            peers += 1

    def meet():
        pl.semaphore_wait(barrier, peers)
        fetches[0].wait()

    stream, choice, mix = meeting
    mixer_body(
        size,
        sides,
        block,
        capacity,
        *mixer_in[:8],
        big_v[0],
        *mixer_in[8:],
        meet,
        stream,
        choice,
        mix,
        *mixer_scratch,
    )
    moe_body(
        sides,
        size,
        capacity,
        block,
        fetches[1:],
        choice,
        stream,
        mix,
        out,
        *moe_scratch[:-17],
        *big_v[1:],
        *moe_scratch[-17:],
    )


def layer(mixer_in, big, block, capacity):
    sides = lax.axis_size("tp")
    groups = lax.axis_size("sp")
    rows, width_in = mixer_in[0].shape
    tokens, width = mixer_in[8].shape
    lanes = 2 * HEAD
    pairs = width_in // lanes
    chunks = rows // BLOCK_SPAN
    close = min(CLOSE, groups)
    half = sides // 2
    f32, b16 = jnp.float32, jnp.bfloat16
    dma = pltpu.SemaphoreType.DMA
    vmem = pltpu.VMEM
    anywhere = pl.BlockSpec(memory_space=pl.ANY)
    slots = groups * block
    mixer_scratch = [
        vmem((rows, width_in), f32),
        vmem((rows, width_in), f32),
        vmem((chunks, pairs, BLOCK_SPAN, 2 * lanes), b16),
        vmem((chunks, pairs, BLOCK_SPAN, 2 * lanes), b16),
        vmem((chunks, pairs, lanes, lanes), f32),
        vmem((chunks, pairs, HEAD, lanes), f32),
        vmem((rows, width_in), f32),
        vmem((rows, width_in), b16),
        vmem((pairs, lanes, lanes), f32),
        vmem((pairs, lanes, lanes), f32),
        vmem((8, lanes), f32),
        vmem((8, lanes), f32),
        vmem((8, lanes), f32),
        vmem((pairs, HEAD, lanes), b16),
        vmem((pairs, HEAD, lanes), b16),
        vmem((pairs, HEAD, lanes), f32),
        vmem((pairs, HEAD, lanes), f32),
        vmem((pairs, HEAD, lanes), b16),
        vmem((pairs, HEAD, lanes), b16),
        vmem((sides, tokens, width), b16),
        vmem((half, tokens, width), b16),
        vmem((half - 1, tokens, width), b16),
        vmem((half - 1, tokens, width), b16),
        dma((2,)),
        dma((2, pairs)),
        dma((2, pairs)),
        dma((pairs,)),
        dma((pairs,)),
        dma((pairs,)),
        dma((2, half)),
        dma((2, half, tokens // 16)),
    ]
    moe_scratch = (
        [
            vmem((groups, block, width), b16),
            vmem((close, half, block, width), b16),
            vmem((half - 1, groups, block, width), b16),
            vmem((half - 1, slots, tokens), f32),
            vmem((half - 1, close, block, width), b16),
            vmem((sides, groups, block, width), b16),
            vmem((sides, tokens, width), b16),
            vmem((sides, groups, block, width), b16),
            vmem((half, groups, block, width), b16),
            vmem((half - 1, groups, block, width), b16),
            vmem((half - 1, groups, block, width), b16),
            vmem((groups, block, width), b16),
            vmem((groups, block, width), b16),
            vmem((sides, 1, tokens, width), b16),
            vmem((half, 1, tokens, width), b16),
            vmem((half - 1, 1, tokens, width), b16),
            vmem((half - 1, 1, tokens, width), b16),
        ]
        + [dma((2,)), dma((groups, half)), dma((groups, half))]
        + [dma((groups + 1,))] * 2
        + [dma((groups + 1, half))] * 8
        + [dma((groups, half))] * 2
        + [dma((half,))] * 2
    )
    counts = (len(mixer_scratch), len(moe_scratch))
    return pl.pallas_call(
        lambda *refs: layer_kernel(groups, sides, block, capacity, counts, *refs),
        out_shape=jax.ShapeDtypeStruct((tokens, width), b16),
        in_specs=[VMEM] * 12 + [anywhere] * 7,
        out_specs=VMEM,
        scratch_shapes=[vmem(w.shape, b16) for w in big]
        + [dma((7,))]
        + [vmem((tokens, width), b16), vmem((sides, slots, tokens), f32), vmem((slots, tokens), f32)]
        + mixer_scratch
        + moe_scratch,
        compiler_params=pltpu.CompilerParams(
            collective_id=1, has_side_effects=True, vmem_limit_bytes=67_000_000
        ),
    )(*mixer_in, *big)


def per_device(
    head_queries,
    head_keys,
    head_values,
    decay_logits,
    learning_logits,
    surge_decay,
    documents,
    residual,
    head_norm_scale,
    mixer_output_weight,
    layer_norm_scale,
    routes,
    routing_weight,
    routed_gate_weight,
    routed_up_weight,
    routed_down_weight,
    common_gate_weight,
    common_up_weight,
    common_down_weight,
):
    groups = lax.axis_size("sp")
    experts = EXP_DEV * groups
    capacity = max(2, (3 * TOK_DEV * TOP + 2 * experts - 1) // (2 * experts))
    block_rows = 8 * ((EXP_DEV * capacity + 7) // 8)
    mixer_in = (
        head_queries,
        head_keys,
        head_values,
        decay_logits,
        learning_logits.T,
        surge_decay.T,
        documents.reshape(1, -1),
        head_norm_scale.reshape(1, -1),
        residual,
        layer_norm_scale.reshape(1, -1),
        routes.T,
        routing_weight.T,
    )
    big = (
        mixer_output_weight,
        common_gate_weight,
        common_up_weight,
        common_down_weight,
        routed_gate_weight,
        routed_up_weight,
        routed_down_weight,
    )
    return layer(mixer_in, big, block_rows, capacity)


def solution(mesh):
    placed = (
        P("sp", "tp"),
        P("sp", "tp"),
        P("sp", "tp"),
        P("sp", "tp"),
        P("sp", "tp"),
        P("sp", "tp"),
        P("sp"),
        P(("sp", "tp"), None),
        P("tp"),
        P("tp", None),
        P(),
        P("sp", None),
        P(("sp", "tp"), None),
        P("sp", None, "tp"),
        P("sp", None, "tp"),
        P("sp", "tp", None),
        P(None, "tp"),
        P(None, "tp"),
        P("tp", None),
    )
    return jax.shard_map(
        per_device, mesh=mesh, in_specs=placed, out_specs=P(("sp", "tp"), None), check_vma=False
    )
```

```python
import jax
import jax.numpy as jnp
from jax import lax
from jax.experimental import pallas as pl
from jax.experimental.pallas import tpu as pltpu
from jax.sharding import PartitionSpec as P

HEAD = 64
EXP_DEV = 2
TOP = 2
BLOCK_SPAN = 64
TOK_DEV = 64


residual_scale = 2.0**0.5
group_eps = 0.00064
norm_eps = 1e-05
unit_eps = 1e-06
CLOSE_PLACE = 3
EXTRA_TURN = 8
NEAR_TURN = 1
LEAD = 5


MESH = pl.DeviceIdType.MESH
VMEM = pl.BlockSpec(memory_space=pltpu.VMEM)


def remote(src, dst, send_sem, recv_sem, axis, index):
    return pltpu.make_async_remote_copy(
        src_ref=src,
        dst_ref=dst,
        send_sem=send_sem,
        recv_sem=recv_sem,
        device_id={axis: index},
        device_id_type=MESH,
    )


def chunk_iota(rows, cols, dim):
    return lax.broadcasted_iota(jnp.int32, (rows, cols), dim)


def mm(left, right, precision=None):
    return jnp.dot(left, right, preferred_element_type=jnp.float32, precision=precision)


def mm_nt(left, right, precision=None):
    return lax.dot_general(
        left,
        right,
        (((1,), (1,)), ((), ())),
        preferred_element_type=jnp.float32,
        precision=precision,
    )


def mm_tn(left, right, precision=None):
    return lax.dot_general(
        left,
        right,
        (((0,), (0,)), ((), ())),
        preferred_element_type=jnp.float32,
        precision=precision,
    )


def narrow(values):
    return values.astype(jnp.bfloat16)


def split(values):
    top = narrow(values)
    return top, narrow(values - top.astype(jnp.float32))


def assign_slots(
    size, sides, block, capacity, rows, tokens, own_tp, routes, route_weight, choice, mix
):
    experts = EXP_DEV * size
    slot_list = size * block
    named = routes[...].astype(jnp.float32)
    expert_row = chunk_iota(experts, rows, 0).astype(jnp.float32)
    taken = jnp.zeros((experts, rows), jnp.float32)
    for route in range(TOP):
        taken = taken + (named[route : route + 1] == expert_row).astype(jnp.float32)
    same_block = (chunk_iota(rows, rows, 0) // tokens) == (chunk_iota(rows, rows, 1) // tokens)
    prior = ((chunk_iota(rows, rows, 0) < chunk_iota(rows, rows, 1)) & same_block).astype(
        jnp.bfloat16
    )
    taken = narrow(taken)
    rank = narrow(mm(taken, prior))
    place = lax.rem(chunk_iota(slot_list, experts, 0), block)
    hosts = ((chunk_iota(slot_list, experts, 0) // block) * EXP_DEV + place // capacity) == (
        chunk_iota(slot_list, experts, 1)
    )
    hosts = (hosts & (place < EXP_DEV * capacity)).astype(jnp.float32)
    seat = lax.rem(lax.rem(chunk_iota(slot_list, rows, 0), block), capacity).astype(jnp.float32)
    chosen = narrow(
        jnp.where(
            (mm(narrow(hosts), taken) > 0.5) & (mm(narrow(hosts), rank) == seat), 1.0, 0.0
        )
    )

    def part_of(who):
        return (
            chunk_iota(rows, tokens, 0) == who * tokens + chunk_iota(rows, tokens, 1)
        ).astype(jnp.bfloat16)

    for who in range(sides):
        choice[who] = mm(chosen, part_of(who))
    named_own = mm(narrow(named), part_of(own_tp))
    expert_own = chunk_iota(experts, tokens, 0).astype(jnp.float32)
    amount = jnp.zeros((experts, tokens), jnp.float32)
    for route in range(TOP):
        amount = amount + jnp.where(
            named_own[route : route + 1] == expert_own, route_weight[route : route + 1, :], 0.0
        )
    mix[...] = choice[own_tp] * mm(hosts, amount, lax.Precision.HIGHEST)


def mixer_body(
    size,
    sides,
    block,
    capacity,
    queries,
    keys,
    values,
    decays,
    rates,
    surges,
    docs,
    scale,
    out_weight,
    residual,
    layer_scale,
    routes,
    route_weight,
    meet,
    stream,
    choice,
    mix,
    ahead_s,
    fwd_s,
    reads_s,
    solved_s,
    map_s,
    add_s,
    local_s,
    starts_s,
    comp_s,
    far_s,
    join_s,
    doc_out,
    doc_in,
    padd_out,
    padd_in,
    pmap_out,
    pmap_in,
    s_out,
    s_in,
    mixed,
    mixed_near,
    mixed_pair,
    mixed_far,
    doc_sem,
    padd_sem,
    pmap_sem,
    near_sem,
    next_sem,
    s_recv,
    mn_sem,
    mf_sem,
):
    me = lax.axis_index("sp")
    span = BLOCK_SPAN
    rows, width = queries.shape
    chunks = rows // span
    lanes = 2 * HEAD
    pairs = width // lanes
    heads = rates.shape[0]
    high = lax.Precision.HIGH
    same_half = (chunk_iota(lanes, lanes, 0) // HEAD) == (chunk_iota(lanes, lanes, 1) // HEAD)
    ones_half = same_half.astype(jnp.float32)
    earlier = lax.rem(chunk_iota(span, lanes, 1), HEAD)
    later = chunk_iota(span, lanes, 0)
    unit_pair = (earlier == later).astype(jnp.float32)
    unit_full = (chunk_iota(lanes, lanes, 0) == chunk_iota(lanes, lanes, 1)).astype(jnp.float32)

    def wide(block):
        return jnp.where(same_half, jnp.concatenate([block, block], 0), 0.0)

    row_docs = docs[...].astype(jnp.float32)
    row_square = jnp.broadcast_to(row_docs, (rows, rows))
    diag = chunk_iota(rows, rows, 0) == chunk_iota(rows, rows, 1)
    doc_col = mm(
        narrow(jnp.where(diag, row_square, 0.0)), jnp.ones((rows, lanes), jnp.bfloat16)
    )
    pick = (
        lax.rem(chunk_iota(rows, lanes, 0), span) == lax.rem(chunk_iota(rows, lanes, 1), HEAD)
    ).astype(jnp.bfloat16)
    wide_rows = 8 * ((chunks + 7) // 8)
    in_chunk = (chunk_iota(wide_rows, rows, 1) // span) == chunk_iota(wide_rows, rows, 0)
    doc_row = mm(
        narrow(jnp.where(in_chunk, jnp.broadcast_to(row_docs, (wide_rows, rows)), 0.0)), pick
    )
    same_chunk = (chunk_iota(rows, rows, 0) // span) == (chunk_iota(rows, rows, 1) // span)
    tri = (
        (chunk_iota(rows, rows, 0) >= chunk_iota(rows, rows, 1)) & same_chunk
    ).astype(jnp.bfloat16)

    strict, causal, joined, tail = [], [], [], []
    for c in range(chunks):
        col = doc_col[c * span : (c + 1) * span]
        same_doc = col == doc_row[c : c + 1]
        strict.append(same_doc & (later > earlier))
        causal.append(same_doc & (later >= earlier))
        before_row = doc_col[max(c * span - 1, 0) : max(c * span - 1, 0) + 1]
        joined.append((col == before_row).astype(jnp.float32))
        tail.append((col == doc_col[(c + 1) * span - 1 : (c + 1) * span]).astype(jnp.float32))

    doc_out[...] = jnp.broadcast_to(doc_col[rows - 1 : rows], doc_out.shape)
    meet()
    following = lax.rem(me + 1, size)
    doc_hop = remote(doc_out, doc_in, doc_sem.at[0], doc_sem.at[1], "sp", following)

    @pl.when(me < size - 1)
    def _():
        doc_hop.start()

    rate_all = jax.nn.sigmoid(rates[...].astype(jnp.float32))
    surge_all = surges[...]

    def local_pairs(turn, carry):
        streams = []
        for half in range(2):
            p = turn * 2 + half
            cols = pl.ds(pl.multiple_of(p * lanes, lanes), lanes)
            spread_heads = (
                chunk_iota(heads, lanes, 0) == 2 * p + chunk_iota(heads, lanes, 1) // HEAD
            ).astype(jnp.float32)
            key = keys[:, cols].astype(jnp.float32)
            norm = mm(key * key, ones_half, high)
            unit = key * lax.rsqrt(norm + unit_eps)
            rate = mm_tn(rate_all, spread_heads, high)
            surge = mm_tn(surge_all, spread_heads, high)
            logit = decays[:, cols].astype(jnp.float32)
            decay = surge - jnp.exp(-0.5) / (1.0 + jnp.exp(-logit))
            top, rest = split(decay)
            cumulative = mm(tri, top) + mm(tri, rest)
            grown = jnp.exp(cumulative)
            shrunk = jnp.exp(-cumulative)
            ahead = unit * jnp.exp(cumulative - decay)
            unit_rate = unit * rate
            back_unit = unit_rate * shrunk
            back_key = key * shrunk
            forward = queries[:, cols].astype(jnp.float32) * grown
            ahead_s[:, cols] = ahead
            fwd_s[:, cols] = forward
            for c in range(chunks):
                part = slice(c * span, (c + 1) * span)
                total = cumulative[(c + 1) * span - 1 : (c + 1) * span]
                ending = jnp.exp(total - cumulative[part]) * tail[c]
                streams.append(
                    dict(
                        c=c,
                        p=p,
                        cols=cols,
                        ahead=ahead[part],
                        fwd=forward[part],
                        bu=back_unit[part],
                        bk=back_key[part],
                        eu=-unit_rate[part] * ending,
                        ek=key[part] * ending,
                        val=values[part, cols].astype(jnp.float32),
                        keep=jnp.exp(total) * joined[c][span - 1 : span],
                    )
                )
        for s in streams:
            c = s["c"]
            scores = mm_nt(
                jnp.concatenate([s["ahead"], s["fwd"]], 0),
                jnp.concatenate([wide(s["bu"]), wide(s["bk"])], 0),
                high,
            )
            s["low"] = jnp.where(strict[c], scores[:span, :lanes], 0.0)
            s["mixk"] = jnp.where(strict[c], scores[:span, lanes:], 0.0)
            reads_s[c, s["p"], :, :lanes] = narrow(
                jnp.where(causal[c], -scores[span:, :lanes], 0.0)
            )
            reads_s[c, s["p"], :, lanes:] = narrow(jnp.where(causal[c], scores[span:, lanes:], 0.0))
        base = 16
        near_block = (earlier // base) == (later // base)
        for s in streams:
            s["low_near"] = jnp.where(near_block, s["low"], 0.0)
            s["inv"] = unit_pair - s["low_near"]
        for s in streams:
            s["power"] = mm(s["low_near"], wide(s["low_near"]), high)
            s["mv"] = mm(s["mixk"], wide(s["val"]))
        reach = 2
        while reach < base:
            last = reach * 2 >= base
            for s in streams:
                right = wide(s["power"])
                if last:
                    s["inv"] = s["inv"] + mm(s["inv"], right, high)
                else:
                    both = mm(jnp.concatenate([s["power"], s["inv"]], 0), right, high)
                    s["power"] = both[:span]
                    s["inv"] = s["inv"] + both[span:]
            reach = reach * 2
        while base < span:
            off = ((earlier // base) != (later // base)) & (
                (earlier // (2 * base)) == (later // (2 * base))
            )
            for s in streams:
                s["mid"] = mm(s["inv"], wide(jnp.where(off, s["low"], 0.0)), high)
            for s in streams:
                s["inv"] = s["inv"] - mm(s["mid"], wide(s["inv"]), high)
            base = base * 2
        for s in streams:
            c = s["c"]
            s["solved"] = mm(
                s["inv"],
                jnp.concatenate([wide(s["ahead"] * joined[c]), wide(s["mv"])], 1),
                high,
            )
            solved_s[c, s["p"]] = narrow(s["solved"])
        for s in streams:
            c, p = s["c"], s["p"]
            pull = mm_tn(s["solved"][:, :lanes], s["eu"], high)
            map_s[c, p] = jnp.where(same_half, pull, 0.0) + unit_full * s["keep"]
            grown = mm_tn(
                jnp.concatenate([s["solved"][:, lanes:], s["val"]], 0),
                jnp.concatenate([s["eu"], s["ek"]], 0),
                high,
            )
            grown = jnp.where(same_half, grown, 0.0)
            add_s[c, p] = grown[:HEAD] + grown[HEAD:]
        return carry

    lax.fori_loop(0, pairs // 2, local_pairs, 0)

    state = [None] * pairs
    for p in range(pairs):
        state[p] = jnp.concatenate([add_s[0, p], map_s[0, p][:HEAD] + map_s[0, p][HEAD:]], 0)
    kept = [state]
    for c in range(1, chunks):
        state = [
            mm(kept[-1][p], map_s[c, p], high)
            + jnp.concatenate([add_s[c, p], jnp.zeros((HEAD, lanes), jnp.float32)], 0)
            for p in range(pairs)
        ]
        kept.append(state)
    finals = kept[-1]

    @pl.when(me == 0)
    def _():
        join_s[...] = jnp.zeros_like(join_s)
        s_in[...] = jnp.zeros_like(s_in)

    @pl.when(me > 0)
    def _():
        doc_hop.wait_recv()
        join_s[...] = (doc_in[...] == doc_col[0:1]).astype(jnp.float32)

    join = join_s[0:1]
    for p in range(pairs):
        comp_s[p] = jnp.concatenate([finals[p][:HEAD], finals[p][HEAD:] * join], 0)
    even = lax.rem(me, 2) == 0

    def pair_hop(p):
        return (
            remote(padd_out.at[p], padd_in.at[p], padd_sem.at[0, p], padd_sem.at[1, p], "sp", following),
            remote(pmap_out.at[p], pmap_in.at[p], pmap_sem.at[0, p], pmap_sem.at[1, p], "sp", following),
        )

    def state_hop(p, near):
        sem = near_sem if near else next_sem
        return remote(
            s_out.at[p],
            s_in.at[p],
            sem.at[p],
            s_recv.at[p],
            "sp",
            lax.rem(me + (2 if near else 1), size),
        )

    @pl.when(even)
    def _():
        for p in range(pairs):
            padd_out[p] = narrow(comp_s[p, :HEAD])
            pmap_out[p] = comp_s[p, HEAD:]
        for p in range(pairs):
            pair_hop(p)[0].start()
        for p in range(pairs):
            pair_hop(p)[1].start()

    def finish_local():
        for p in range(pairs):
            cols = slice(p * lanes, (p + 1) * lanes)
            for c in range(chunks):
                part = slice(c * span, (c + 1) * span)
                read_unit = reads_s[c, p, :, :lanes]
                solved = solved_s[c, p].astype(jnp.float32)
                local = mm(
                    reads_s[c, p],
                    jnp.concatenate(
                        [
                            narrow(wide(solved[:, lanes:])),
                            narrow(wide(values[part, cols].astype(jnp.float32))),
                        ],
                        0,
                    ),
                )
                start = fwd_s[part, cols] * joined[c] + mm(
                    read_unit, narrow(wide(solved[:, :lanes]))
                )
                if c > 0:
                    seen = mm_nt(
                        narrow(start),
                        jnp.concatenate(
                            [
                                narrow(wide(kept[c - 1][p][:HEAD])),
                                narrow(wide(kept[c - 1][p][HEAD:])),
                            ],
                            0,
                        ),
                    )
                    local = local + seen[:, :lanes]
                    start = seen[:, lanes:]
                local_s[part, cols] = local
                starts_s[part, cols] = narrow(start)

    own_tp = lax.axis_index("tp")
    tokens = residual.shape[0]

    def assign():
        assign_slots(
            size, sides, block, capacity, rows, tokens, own_tp, routes, route_weight, choice, mix
        )

    @pl.when(even)
    def _():
        finish_local()
        assign()

    @pl.when(jnp.logical_not(even))
    def _():
        for p in range(pairs):
            pair_hop(p)[0].wait_recv()
            first = padd_in[p]
            top, rest = split(wide(comp_s[p, HEAD:]))
            far_s[p, :HEAD] = (
                mm(jnp.concatenate([first, first], 1), jnp.concatenate([top, rest], 0))
                + comp_s[p, :HEAD]
            )

        @pl.when(me == 1)
        def _():
            s_in[...] = jnp.zeros_like(s_in)
            for p in range(pairs):
                s_out[p] = narrow(far_s[p, :HEAD])
                state_hop(p, True).start()
                state_hop(p, False).start()

        finish_local()

        @pl.when((me == 1) | (me > 3))
        def _():
            assign()

        for p in range(pairs):
            pair_hop(p)[1].wait_recv()

        @pl.when(me > 1)
        def _():
            for p in range(pairs):
                both = mm(pmap_in[p], wide(comp_s[p, HEAD:]), high)
                far_s[p, HEAD:] = both
            weights = []
            for p in range(pairs):
                top, rest = split(wide(far_s[p, HEAD:]))
                weights.append(jnp.concatenate([top, rest], 0))
            for p in range(pairs):
                state_hop(p, True).wait_recv()

                @pl.when(me < size - 1)
                def _():
                    arrived = s_in[p]
                    s_out[p] = narrow(
                        mm(jnp.concatenate([arrived, arrived], 1), weights[p]) + far_s[p, :HEAD]
                    )
                    state_hop(p, True).start()

            @pl.when(me < size - 1)
            def _():
                for p in range(pairs):
                    state_hop(p, False).start()

            @pl.when(me == 3)
            def _():
                assign()

        for p in range(pairs):
            top, rest = split(wide(pmap_in[p]))
            arrived = s_in[p]
            comp_s[p, :HEAD] = (
                mm(jnp.concatenate([arrived, arrived], 1), jnp.concatenate([top, rest], 0))
                + padd_in[p].astype(jnp.float32)
            )

    @pl.when(even)
    def _():
        @pl.when(me > 0)
        def _():
            for p in range(pairs):
                state_hop(p, False).wait_recv()

        for p in range(pairs):
            comp_s[p, :HEAD] = s_in[p].astype(jnp.float32)

    half = sides // 2
    partner = own_tp + 1 - 2 * lax.rem(own_tp, 2)
    split_rows = 16
    split_list = tokens // split_rows

    def ahead(j, who=None):
        return lax.rem((own_tp if who is None else who) + 2 * j, sides)

    def near_hop(j):
        return remote(
            mixed.at[ahead(j, partner)], mixed_near.at[j], mn_sem.at[0, j], mn_sem.at[1, j], "tp", partner
        )

    def far_hop(j, i):
        span_rows = pl.ds(i * split_rows, split_rows)
        return remote(
            mixed_pair.at[j - 1, span_rows],
            mixed_far.at[j - 1, span_rows],
            mf_sem.at[0, j, i],
            mf_sem.at[1, j, i],
            "tp",
            ahead(j),
        )

    incoming = [narrow(wide(comp_s[p, :HEAD] * join)) for p in range(pairs)]

    def project(quarters):
        parts = [pl.ds(pl.multiple_of(q * tokens, tokens), tokens) for q in quarters]
        normed = []
        for p in range(pairs):
            cols = slice(p * lanes, (p + 1) * lanes)
            read = jnp.concatenate([local_s[part, cols] for part in parts], 0) + mm_nt(
                jnp.concatenate([starts_s[part, cols] for part in parts], 0), incoming[p]
            )
            centred = read - mm(read, ones_half, high) * (1.0 / HEAD)
            spread = mm(centred * centred, ones_half, high) * (1.0 / HEAD)
            normed.append(
                narrow(centred * lax.rsqrt(spread + group_eps) * scale[:, cols])
            )
        product = narrow(mm(jnp.concatenate(normed, 1), out_weight[...]))
        for i, quarter in enumerate(quarters):
            mixed[quarter] = product[i * tokens : (i + 1) * tokens]

    for j in range(half - 1, -1, -1):
        project([ahead(j, partner), ahead(j)])
        near_hop(j).start()
        if j > 0:
            near_hop(j).wait_recv()
            for i in range(split_list):
                take = slice(i * split_rows, (i + 1) * split_rows)
                mixed_pair[j - 1, take] = narrow(
                    mixed[ahead(j), take].astype(jnp.float32)
                    + mixed_near[j, take].astype(jnp.float32)
                )
                far_hop(j, i).start()
    near_hop(0).wait_recv()
    for i in range(split_list):
        take = slice(i * split_rows, (i + 1) * split_rows)
        total = (
            residual_scale * residual[take].astype(jnp.float32)
            + mixed[own_tp, take].astype(jnp.float32)
            + mixed_near[0, take].astype(jnp.float32)
        )
        for j in range(1, half):
            far_hop(j, i).wait_recv()
            total = total + mixed_far[j - 1, take].astype(jnp.float32)
        centred = total - jnp.mean(total, -1, keepdims=True)
        spread = jnp.mean(centred * centred, -1, keepdims=True)
        stream[take] = narrow(centred * lax.rsqrt(spread + norm_eps) * layer_scale[...])

    for j in range(half):
        near_hop(j).wait_send()
        if j > 0:
            for i in range(split_list):
                far_hop(j, i).wait_send()

    @pl.when(me < size - 1)
    def _():
        doc_hop.wait_send()

    @pl.when(even)
    def _():
        for p in range(pairs):
            for hop in pair_hop(p):
                hop.wait_send()

    @pl.when(jnp.logical_not(even) & (me < size - 1))
    def _():
        for p in range(pairs):
            state_hop(p, True).wait_send()
            state_hop(p, False).wait_send()


def flip(index, bits, size):
    total = 0
    place = 1
    while place < size:
        total = total + lax.rem(lax.div(index, place) + lax.div(bits, place), 2) * place
        place = place * 2
    return total


def piece(position, groups):
    later = lax.div(lax.div(position, 4) + groups, groups + 1)
    early = (1 + lax.rem(position, 3)) * lax.div(position + 3, 4)
    return later * position + (1 - later) * early


def moe_body(
    size,
    groups,
    capacity,
    block,
    fetches,
    choice,
    stream,
    mix,
    out,
    outgoing,
    near_out,
    returned_far,
    mix_far,
    stage_far,
    arrived,
    rows_all,
    parts,
    near,
    pair,
    far,
    stage,
    returned,
    extra,
    enear,
    epair,
    efar,
    cgate_v,
    cup_v,
    cdown_v,
    gate_v,
    up_v,
    down_v,
    local,
    asend,
    arecv,
    nsend,
    nrecv,
    fsend,
    frecv,
    gsend,
    grecv,
    rnsend,
    rnrecv,
    rfsend,
    rfrecv,
    bsend,
    brecv,
    msend,
    mrecv,
):
    me = lax.axis_index("tp")
    own = lax.axis_index("sp")
    half = size // 2
    partner = me + 1 - 2 * lax.rem(me, 2)
    tokens, width = stream.shape
    batch = max(1, groups // 8)
    steps = groups // batch
    keep_rows = pltpu.make_async_copy(stream, rows_all.at[me], local.at[1])
    keep_rows.start()
    def ahead(j):
        return lax.rem(me + 2 * j, size)

    def exchange(k, j=0, near=False):
        other = flip(own, piece(k, groups), groups)
        return remote(
            near_out.at[j] if near else outgoing.at[other],
            arrived.at[ahead(j), k],
            asend.at[k, j],
            arecv.at[k, j],
            "sp",
            other,
        )

    def send_mix(j):
        return remote(mix, mix_far.at[j - 1], msend.at[j], mrecv.at[j], "tp", ahead(size - j))

    def place(k, who, whole):
        return rows_all.at[who] if whole else arrived.at[who, k]

    def near_copy(k, whole=False):
        src = stream if whole else arrived.at[me, k]
        return remote(src, place(k, me, whole), nsend.at[k], nrecv.at[k], "tp", partner)

    def far_copy(k, j, whole=False):
        src = stream if whole else arrived.at[me, k]
        return remote(
            src, place(k, me, whole), fsend.at[k, j], frecv.at[k, j], "tp", lax.rem(me + 2 * j, size)
        )

    def forward(k, j, whole=False):
        ref = place(k, lax.rem(me - 2 * j + size, size), whole)
        return remote(ref, ref, gsend.at[k, j], grecv.at[k, j], "tp", partner)

    def send_own(k, whole=False):
        for j in range(1, half):
            far_copy(k, j, whole).start()
        near_copy(k, whole).start()

    def pass_on(k, whole=False):
        for j in range(1, half):
            far_copy(k, j, whole).wait_recv()
            forward(k, j, whole).start()

    def gathered(k, whole=False):
        near_copy(k, whole).wait_recv()
        for j in range(1, half):
            forward(k, j, whole).wait_recv()

    def reduce_near(k, j, whole=False):
        src, dst = (extra, enear) if whole else (parts, near)
        index = 0 if whole else k
        return remote(
            src.at[lax.rem(partner + 2 * j, size), index],
            dst.at[j, index],
            rnsend.at[k, j],
            rnrecv.at[k, j],
            "tp",
            partner,
        )

    def reduce_far(k, j, whole=False):
        src, dst = (epair, efar) if whole else (pair, far)
        index = 0 if whole else k
        return remote(
            src.at[j - 1, index],
            dst.at[j - 1, index],
            rfsend.at[k, j],
            rfrecv.at[k, j],
            "tp",
            lax.rem(me + 2 * j, size),
        )

    def back(k, j=0, whose=None):
        other = flip(own, piece(k, groups), groups)
        where = own if whose is None else whose
        return remote(
            stage.at[k] if j == 0 else stage_far.at[j - 1],
            returned.at[where] if j == 0 else returned_far.at[j - 1, where],
            bsend.at[k, j],
            brecv.at[k, j],
            "sp",
            other,
        )

    def finish_close(k):
        for j in range(half):
            reduce_near(k, j).wait_recv()
            total = narrow(
                parts[ahead(j), k].astype(jnp.float32) + near[j, k].astype(jnp.float32)
            )

            @pl.when(k == 0)
            def _():
                if j == 0:
                    returned[own] = total
                else:
                    returned_far[j - 1, own] = total

            @pl.when(k > 0)
            def _():
                if j == 0:
                    stage[k] = total
                else:
                    stage_far[j - 1] = total
                back(k, j).start()

    def weighed(weights, rows):
        top, rest = split(weights)
        rows = narrow(rows.astype(jnp.float32).reshape(groups * block, width))
        return mm_tn(top, rows) + mm_tn(rest, rows)

    def add_extra():
        k = CLOSE_PLACE
        for j in range(half):
            back(k, j, flip(own, piece(k, groups), groups)).wait_recv()
        for j in range(1, half):
            reduce_near(groups, j, True).wait_recv()
            send_mix(j).wait_recv()
            epair[j - 1, 0] = narrow(
                extra[ahead(j), 0].astype(jnp.float32)
                + enear[j, 0].astype(jnp.float32)
                + weighed(mix_far[j - 1], returned_far[j - 1])
            )
            reduce_far(groups, j, True).start()

    def start_reduce(k, whole=False):
        for j in range(half - 1, -1, -1):
            reduce_near(k, j, whole).start()

    def add_pair(k, whole=False):
        src, got, to = (extra, enear, epair) if whole else (parts, near, pair)
        index = 0 if whole else k
        for j in range(1, half):
            reduce_near(k, j, whole).wait_recv()
            to[j - 1, index] = narrow(
                src[lax.rem(me + 2 * j, size), index].astype(jnp.float32)
                + got[j, index].astype(jnp.float32)
            )
            reduce_far(k, j, whole).start()

    def total_of(k, whole=False):
        src, got, last = (extra, enear, efar) if whole else (parts, near, far)
        index = 0 if whole else k
        reduce_near(k, 0, whole).wait_recv()
        total = src[me, index].astype(jnp.float32) + got[0, index].astype(jnp.float32)
        for j in range(1, half):
            reduce_far(k, j, whole).wait_recv()
            total = total + last[j - 1, index].astype(jnp.float32)
        return total

    def swish(gated, lifted):
        return gated / (1.0 + jnp.exp(-gated)) * lifted

    lead, relay = min(LEAD, steps), min(2, steps)

    def send_pieces(low, high):
        for k in range(max(1, low), min(high, groups)):
            if k != CLOSE_PLACE:
                exchange(k).wait_recv()
                send_own(k)

    send_own(groups, True)
    outgoing[...] = narrow(mm(narrow(choice[me]), stream[...])).reshape(groups, block, width)
    for k in range(1, groups):
        if k != CLOSE_PLACE:
            exchange(k).start()
    for j in range(1, half):
        send_mix(j).start()
    send_pieces(1, 4 * batch)
    keep_rows.wait()
    pass_on(groups, True)
    other = flip(own, piece(CLOSE_PLACE, groups), groups)
    for j in range(half):
        picked = narrow(choice[ahead(j), pl.ds(pl.multiple_of(other * block, 8), block)])
        near_out[j] = narrow(mm(picked, rows_all[ahead(j)]))
        exchange(CLOSE_PLACE, j, True).start()
    send_pieces(4 * batch, 5 * batch)
    gathered(groups, True)
    for who in range(size):
        picked = narrow(choice[who, pl.ds(pl.multiple_of(own * block, 8), block)])
        arrived[who, 0] = narrow(mm(picked, rows_all[who]))
    for fetch in fetches[:3]:
        fetch.wait()
    everyone = rows_all[...].reshape(size * tokens, width)
    hidden = narrow(swish(mm(everyone, cgate_v[...]), mm(everyone, cup_v[...])))
    send_pieces(5 * batch, (lead + 1) * batch)
    extra[...] = narrow(mm(hidden, cdown_v[...])).reshape(size, 1, tokens, width)
    start_reduce(groups, True)
    for k in range(1, relay * batch):
        if k != CLOSE_PLACE:
            pass_on(k)
    for fetch in fetches[3:]:
        fetch.wait()

    def near_arrive():
        k = CLOSE_PLACE
        for j in range(half):
            exchange(k, j, True).wait_recv()
        near_copy(k).start()
        for j in range(1, half):
            forward(k, j).start()

    if batch > 1:
        near_arrive()

    piece_rows = size * batch * block
    row = lax.broadcasted_iota(jnp.int32, (piece_rows, gate_v.shape[2]), 0)
    hosted = lax.div(lax.rem(row, block), capacity)

    def turn(t, carry):
        def each(base, action):
            for b in range(batch):
                action(base * batch + b)

        @pl.when((t > 0) & (t + lead < steps))
        def _():
            def action(k):
                exchange(k).wait_recv()
                send_own(k)

            each(t + lead, action)

        @pl.when(t + relay < steps)
        def _():
            def relay_piece(k):
                @pl.when(k != CLOSE_PLACE)
                def _():
                    pass_on(k)

            each(t + relay, relay_piece)

        @pl.when(t < steps)
        def _():
            def arrive(k):
                @pl.when(k > 0)
                def _():
                    gathered(k)

            each(t, arrive)
            rows_in = narrow(
                arrived[:, pl.ds(t * batch, batch)].astype(jnp.float32).reshape(piece_rows, width)
            )
            hidden = []
            for expert in range(EXP_DEV):
                gated = mm(rows_in, gate_v[expert])
                lifted = mm(rows_in, up_v[expert])
                hidden.append(narrow(jnp.where(hosted == expert, swish(gated, lifted), 0.0)))
            part = mm(jnp.concatenate(hidden, 1), down_v[...].reshape(-1, width))
            parts[:, pl.ds(t * batch, batch)] = narrow(
                part.reshape(size, batch, block, width)
            )
            each(t, start_reduce)

        if batch == 1:

            @pl.when(t == NEAR_TURN)
            def _():
                near_arrive()

        @pl.when((t >= 1) & (t <= steps))
        def _():
            def action(k):
                @pl.when((k == 0) | (k == CLOSE_PLACE))
                def _():
                    finish_close(k)

                @pl.when((k > 0) & (k != CLOSE_PLACE))
                def _():
                    add_pair(k)

            each(t - 1, action)

        @pl.when(t == min(EXTRA_TURN, steps + 1))
        def _():
            add_extra()

        @pl.when(t >= 2)
        def _():
            def action(k):
                @pl.when((k > 0) & (k != CLOSE_PLACE))
                def _():
                    stage[k] = narrow(total_of(k))
                    back(k).start()

            each(t - 2, action)

        return carry

    lax.fori_loop(0, steps + 2, turn, 0)

    shared = total_of(groups, True)
    for k in range(1, groups):
        if k != CLOSE_PLACE:
            back(k, 0, flip(own, piece(k, groups), groups)).wait_recv()
    out[...] = narrow(
        residual_scale * stream[...].astype(jnp.float32)
        + weighed(mix[...], returned[...])
        + shared
    )

    for k in range(1, groups):
        direct = k == CLOSE_PLACE
        for j in range(half if direct else 1):
            exchange(k, j, direct).wait_send()
            back(k, j).wait_send()
    for k in range(groups + 1):
        whole = k == groups
        direct = k in (0, CLOSE_PLACE)
        for j in range(half):
            reduce_near(k, j, whole).wait_send()
        if k > 0:
            near_copy(k, whole).wait_send()
        for j in range(1, half):
            if k > 0:
                forward(k, j, whole).wait_send()
            if not direct:
                far_copy(k, j, whole).wait_send()
                reduce_far(k, j, whole).wait_send()
    for j in range(1, half):
        send_mix(j).wait_send()


def layer_kernel(size, sides, block, capacity, counts, *refs):
    refs = list(refs)

    def take(count):
        got = refs[:count]
        del refs[:count]
        return got

    mixer_in = take(12)
    big = take(7)
    (out,) = take(1)
    big_v = take(7)
    (loads,) = take(1)
    meeting = take(3)
    mixer_scratch = take(counts[0])
    moe_scratch = take(counts[1])
    returned_far = moe_scratch[2]
    fetches = [
        pltpu.make_async_copy(src, dst, loads.at[i]) for i, (src, dst) in enumerate(zip(big, big_v))
    ]
    for fetch in fetches:
        fetch.start()
    returned_far[...] = jnp.zeros_like(returned_far)
    barrier = pltpu.get_barrier_semaphore()
    peers = 0
    for axis, number in (("sp", size), ("tp", sides)):
        here = lax.axis_index(axis)
        for step in range(1, number):
            pl.semaphore_signal(
                barrier,
                inc=1,
                device_id={axis: lax.rem(here + step, number)},
                device_id_type=MESH,
            )
            peers += 1

    def meet():
        pl.semaphore_wait(barrier, peers)
        fetches[0].wait()

    stream, choice, mix = meeting
    mixer_body(
        size,
        sides,
        block,
        capacity,
        *mixer_in[:8],
        big_v[0],
        *mixer_in[8:],
        meet,
        stream,
        choice,
        mix,
        *mixer_scratch,
    )
    moe_body(
        sides,
        size,
        capacity,
        block,
        fetches[1:],
        choice,
        stream,
        mix,
        out,
        *moe_scratch[:-17],
        *big_v[1:],
        *moe_scratch[-17:],
    )


def layer(mixer_in, big, block, capacity):
    sides = lax.axis_size("tp")
    groups = lax.axis_size("sp")
    rows, width_in = mixer_in[0].shape
    tokens, width = mixer_in[8].shape
    lanes = 2 * HEAD
    pairs = width_in // lanes
    chunks = rows // BLOCK_SPAN
    half = sides // 2
    f32, b16 = jnp.float32, jnp.bfloat16
    dma = pltpu.SemaphoreType.DMA
    vmem = pltpu.VMEM
    anywhere = pl.BlockSpec(memory_space=pl.ANY)
    slots = groups * block
    mixer_scratch = [
        vmem((rows, width_in), f32),
        vmem((rows, width_in), f32),
        vmem((chunks, pairs, BLOCK_SPAN, 2 * lanes), b16),
        vmem((chunks, pairs, BLOCK_SPAN, 2 * lanes), b16),
        vmem((chunks, pairs, lanes, lanes), f32),
        vmem((chunks, pairs, HEAD, lanes), f32),
        vmem((rows, width_in), f32),
        vmem((rows, width_in), b16),
        vmem((pairs, lanes, lanes), f32),
        vmem((pairs, lanes, lanes), f32),
        vmem((8, lanes), f32),
        vmem((8, lanes), f32),
        vmem((8, lanes), f32),
        vmem((pairs, HEAD, lanes), b16),
        vmem((pairs, HEAD, lanes), b16),
        vmem((pairs, HEAD, lanes), f32),
        vmem((pairs, HEAD, lanes), f32),
        vmem((pairs, HEAD, lanes), b16),
        vmem((pairs, HEAD, lanes), b16),
        vmem((sides, tokens, width), b16),
        vmem((half, tokens, width), b16),
        vmem((half - 1, tokens, width), b16),
        vmem((half - 1, tokens, width), b16),
        dma((2,)),
        dma((2, pairs)),
        dma((2, pairs)),
        dma((pairs,)),
        dma((pairs,)),
        dma((pairs,)),
        dma((2, half)),
        dma((2, half, tokens // 16)),
    ]
    moe_scratch = (
        [
            vmem((groups, block, width), b16),
            vmem((half, block, width), b16),
            vmem((half - 1, groups, block, width), b16),
            vmem((half - 1, slots, tokens), f32),
            vmem((half - 1, block, width), b16),
            vmem((sides, groups, block, width), b16),
            vmem((sides, tokens, width), b16),
            vmem((sides, groups, block, width), b16),
            vmem((half, groups, block, width), b16),
            vmem((half - 1, groups, block, width), b16),
            vmem((half - 1, groups, block, width), b16),
            vmem((groups, block, width), b16),
            vmem((groups, block, width), b16),
            vmem((sides, 1, tokens, width), b16),
            vmem((half, 1, tokens, width), b16),
            vmem((half - 1, 1, tokens, width), b16),
            vmem((half - 1, 1, tokens, width), b16),
        ]
        + [dma((2,)), dma((groups, half)), dma((groups, half))]
        + [dma((groups + 1,))] * 2
        + [dma((groups + 1, half))] * 8
        + [dma((groups, half))] * 2
        + [dma((half,))] * 2
    )
    counts = (len(mixer_scratch), len(moe_scratch))
    return pl.pallas_call(
        lambda *refs: layer_kernel(groups, sides, block, capacity, counts, *refs),
        out_shape=jax.ShapeDtypeStruct((tokens, width), b16),
        in_specs=[VMEM] * 12 + [anywhere] * 7,
        out_specs=VMEM,
        scratch_shapes=[vmem(w.shape, b16) for w in big]
        + [dma((7,))]
        + [vmem((tokens, width), b16), vmem((sides, slots, tokens), f32), vmem((slots, tokens), f32)]
        + mixer_scratch
        + moe_scratch,
        compiler_params=pltpu.CompilerParams(
            collective_id=1, has_side_effects=True, vmem_limit_bytes=67_000_000
        ),
    )(*mixer_in, *big)


def per_device(
    head_queries,
    head_keys,
    head_values,
    decay_logits,
    learning_logits,
    surge_decay,
    documents,
    residual,
    head_norm_scale,
    mixer_output_weight,
    layer_norm_scale,
    routes,
    routing_weight,
    routed_gate_weight,
    routed_up_weight,
    routed_down_weight,
    common_gate_weight,
    common_up_weight,
    common_down_weight,
):
    groups = lax.axis_size("sp")
    experts = EXP_DEV * groups
    capacity = max(2, (3 * TOK_DEV * TOP + 2 * experts - 1) // (2 * experts))
    block_rows = 8 * ((EXP_DEV * capacity + 7) // 8)
    mixer_in = (
        head_queries,
        head_keys,
        head_values,
        decay_logits,
        learning_logits.T,
        surge_decay.T,
        documents.reshape(1, -1),
        head_norm_scale.reshape(1, -1),
        residual,
        layer_norm_scale.reshape(1, -1),
        routes.T,
        routing_weight.T,
    )
    big = (
        mixer_output_weight,
        common_gate_weight,
        common_up_weight,
        common_down_weight,
        routed_gate_weight,
        routed_up_weight,
        routed_down_weight,
    )
    return layer(mixer_in, big, block_rows, capacity)


def solution(mesh):
    placed = (
        P("sp", "tp"),
        P("sp", "tp"),
        P("sp", "tp"),
        P("sp", "tp"),
        P("sp", "tp"),
        P("sp", "tp"),
        P("sp"),
        P(("sp", "tp"), None),
        P("tp"),
        P("tp", None),
        P(),
        P("sp", None),
        P(("sp", "tp"), None),
        P("sp", None, "tp"),
        P("sp", None, "tp"),
        P("sp", "tp", None),
        P(None, "tp"),
        P(None, "tp"),
        P("tp", None),
    )
    return jax.shard_map(
        per_device, mesh=mesh, in_specs=placed, out_specs=P(("sp", "tp"), None), check_vma=False
    )
```
